256 devices in a mesh: grp: 2 (over z), ep: 64 (over y, x), tp: 2 (over core).
Axes of the slice: x: 8, y: 8, z: 2, core: 2. Of those that a mesh axis runs over, the one named last changes fastest.
The devices are a block of a 8x8x16 slice.
Arguments:
- tokens: bfloat16 [1024, 1536], P(('grp', 'ep')), parts along dimension 0, may hold values from -6 to 6
- norm_gain: float32 [1536], replicated, may hold values from 0.1 to 1.9
- routes: int32 [1024, 4], P(('grp', 'ep')), parts along dimension 0, may hold values from 0 to 63, all different within a row; in each aligned block of 8 rows (0 to 7, 8 to 15, ...) at most 2 rows name the same one
- route_weight: float32 [1024, 4], P(('grp', 'ep')), parts along dimension 0, may hold values from 0.1 to 1
- expert_gate: bfloat16 [64, 1536, 1536], P('ep', None, 'tp'), may hold values from -2 to 2
- expert_up: bfloat16 [64, 1536, 1536], P('ep', None, 'tp'), may hold values from -2 to 2
- expert_down: bfloat16 [64, 1536, 1536], P('ep', 'tp'), may hold values from -0.0390625 to 0.0390625
- dense_gate: bfloat16 [1536, 4096], P(None, ('ep', 'tp')), may hold values from -2 to 2
- dense_up: bfloat16 [1536, 4096], P(None, ('ep', 'tp')), may hold values from -2 to 2
- dense_down: bfloat16 [4096, 1536], P(('ep', 'tp')), may hold values from -0.0234375 to 0.0234375
- gate_vector: bfloat16 [4096], P(('ep', 'tp')), may hold values from -0.0234375 to 0.0234375
Outputs:
- mixed: bfloat16 [1024, 1536], P(('grp', 'ep'), 'tp'), parts along dimension 0
The draws below stay inside these ranges and needn't reach their ends.
There are 2 independent parts, one for each index of `grp`. The reference program is written for one: setup_inputs(seed, part) draws one part's arguments, and reference() takes and returns one part's arrays. A program takes and returns all parts, laid end to end along the dimension named above; an argument that names none is the same for every part. Nothing has to cross between parts.
Inputs may be any that keep to these rules, and one draw needn't show every extreme that they name: `routes`: each token names 4 different experts. Within the rows of one index of ep (aligned blocks of 8 rows) no expert is named by more than 2 rows, a bound that some block reaches.
All inputs are finite; a program needn't handle non-finite values.
Results may differ from the reference program's by a relative error of at most 0.0077.
Values may be sent and summed in bfloat16 or wider, within the bound.
No kernel may reach another device: no remote copies, remote signals or barrier semaphores. Data moves between devices by JAX's collectives and lax.ppermute only.
A program may use at most 64 MiB of HBM per device.

```python
import math
import jax
import jax.numpy as jnp
import numpy as np
from jax import lax

D = 1536
F = 1536
SH = 4096
TOPK = 4
TOK_DEV = 8
EXPERTS = 64
TOKENS = 512
CAP = 2
N_EP = 64
N_TP = 2


def scaled_weight(key, array_shape, fan_in):
    key_base, key_scale = jax.random.split(key)
    normals = jnp.clip(jax.random.normal(key_base, array_shape, jnp.float32), -5.0, 5.0)
    scale_shape = array_shape[:-2] + (1, array_shape[-1])
    low_end, high_end = (1.0, 3.0)
    column_scale = jnp.exp(jax.random.uniform(key_scale, scale_shape, jnp.float32, jnp.log(low_end), jnp.log(high_end)))
    values = jnp.clip(normals * column_scale * fan_in ** (-0.5), -2.0, 2.0)
    return values.astype(jnp.bfloat16)


def draw_expert_gate(key, part):
    return scaled_weight(jax.random.fold_in(key, 11), (EXPERTS, D, F), D)


def draw_expert_up(key, part):
    return scaled_weight(jax.random.fold_in(key, 23), (EXPERTS, D, F), D)


def draw_dense_gate(key, part):
    return scaled_weight(jax.random.fold_in(key, 37), (D, SH), D)


def draw_dense_up(key, part):
    return scaled_weight(jax.random.fold_in(key, 41), (D, SH), D)


def shard_levels(rng, dims, cuts, low, largest):
    loudness, own = 1.0, jax.random.fold_in(rng, 6)
    for position, parts in cuts:
        steps = jnp.exp(jax.random.uniform(jax.random.fold_in(own, position), (parts,), jnp.float32, low / len(cuts), largest / len(cuts)))
        loudness = loudness * jnp.repeat(steps, dims[position] // parts).reshape([-1 if axis == position else 1 for axis in range(len(dims))])
    return loudness


def deal_out(key, own, number, rows, amount, top, reach, skew):
    sequence = jax.random.permutation(key, amount)
    packed, ordinary = shares(amount, rows * top, reach, skew, True), shares(amount, rows * top, reach, skew, False)
    places = jnp.arange(amount)

    def named(tallies, offset_by):
        used = int((tallies > 0).sum())
        fixed = max(1, used // 4)
        passed = fixed + (places - fixed + offset_by * (used - fixed)) % max(1, amount - fixed)
        return jnp.zeros((amount,), jnp.int32).at[sequence[jnp.where(places < fixed, places, passed)]].set(jnp.asarray(tallies, jnp.int32))

    tallies = jnp.where(number % 4 == 0, named(packed, number // 4), named(ordinary, number - number // 4 - 1))
    mixed = jax.random.permutation(jax.random.fold_in(own, 3), amount)
    source_of, receiver = mixed[0:amount // 2 * 2:2], mixed[1:amount // 2 * 2:2]
    slack = jnp.minimum(tallies[source_of] - 1, reach - tallies[receiver]) // 2
    slack = jnp.where((source_of == sequence[0]) | (receiver == sequence[0]) | (tallies[receiver] == 0), 0, jnp.maximum(slack, 0))
    passed = jax.random.randint(jax.random.fold_in(own, 4), (amount // 2,), 0, 1 << 20) % (slack + 1)
    tallies = tallies.at[source_of].add(-passed).at[receiver].add(passed)
    labels = jnp.searchsorted(jnp.cumsum(tallies), jnp.arange(rows * top), side="right").astype(jnp.int32)
    listing = labels.reshape(top, rows).T
    listing = listing[jax.random.permutation(jax.random.fold_in(own, 1), rows)]
    offset_by = jax.random.randint(jax.random.fold_in(own, 2), (rows, 1), 0, top)
    return jnp.take_along_axis(listing, (jnp.arange(top)[None, :] + offset_by) % top, axis=1)


def shares(number_of, total, most, skew, full):
    portions = [(1 << 20) // math.isqrt(grade ** skew) + 1 for grade in range(1, number_of + 1)]
    largest = most if full else min(most, max(-(-total // number_of), total * portions[0] // sum(portions)))
    least = 1 if total - largest >= number_of - 1 else 0
    given, rest = [largest] + [least] * (number_of - 1), total - largest - least * (number_of - 1)
    while rest > 0:
        free = [i for i in range(1, number_of) if given[i] < largest] or [i for i in range(1, number_of) if given[i] < most]
        whole, budget = sum([portions[i] for i in free]), rest
        for i in free:
            more = min(most - given[i], max(1, budget * portions[i] // whole), rest)
            given[i] = given[i] + more
            rest = rest - more
    return np.array(given)


def normal_values(key, extent, scale, limit, shards=(), kind=jnp.bfloat16):
    values = jax.random.normal(key, extent, jnp.float32) * scale
    if len(shards) > 0:
        values = shard_levels(key, extent, shards, -0.22, 0.18) * values
    return jnp.clip(values, min=-limit, max=limit).astype(kind)


def setup_inputs(seed: int = 0, part: int = 0) -> dict:
    keys = jax.random.split(jax.random.key(seed), 12)
    part_keys = jax.random.split(jax.random.fold_in(keys[11], part), 12)
    tokens = normal_values(part_keys[0], (TOKENS, D), 1.0, 6.0, ((0, 64),))
    norm_gain = jnp.clip(1.0 + 0.18 * jax.random.normal(keys[1], (D,), jnp.float32), 0.1, 1.9)
    routes_keys = jax.random.split(jax.random.fold_in(part_keys[2], 1), TOKENS // TOK_DEV)
    routes_turns = jax.random.permutation(jax.random.fold_in(part_keys[2], 3), TOKENS // TOK_DEV)
    routes = jax.vmap(lambda own, number: deal_out(jax.random.fold_in(part_keys[2], 2), own, number, TOK_DEV, EXPERTS, TOPK, CAP, 2))(routes_keys, routes_turns).reshape((TOKENS, TOPK))
    route_weight = jnp.clip(jnp.exp(math.log(1.0) - 2.3025851 * jax.random.uniform(part_keys[3], (TOKENS, TOPK), jnp.float32) ** shard_levels(part_keys[3], (TOKENS, TOPK), ((0, 64),), -0.2, 0.2)), 0.1, 1.0)
    expert_gate = draw_expert_gate(jax.random.fold_in(keys[11], 71), part)
    expert_up = draw_expert_up(jax.random.fold_in(keys[11], 71), part)
    expert_down = normal_values(keys[6], (EXPERTS, F, D), (16 * F) ** -0.5, 0.0390625, ((0, 64), (1, 2)))
    dense_gate = draw_dense_gate(jax.random.fold_in(keys[11], 71), part)
    dense_up = draw_dense_up(jax.random.fold_in(keys[11], 71), part)
    dense_down = normal_values(keys[9], (SH, D), (16 * SH) ** -0.5, 0.0234375, ((0, 128),))
    gate_vector = normal_values(keys[10], (SH,), (16 * SH) ** -0.5, 0.0234375, ((0, 128),))
    return {"tokens": tokens, "norm_gain": norm_gain, "routes": routes, "route_weight": route_weight, "expert_gate": expert_gate, "expert_up": expert_up, "expert_down": expert_down, "dense_gate": dense_gate, "dense_up": dense_up, "dense_down": dense_down, "gate_vector": gate_vector}


clamp_limit = 7.0
sigmoid_slope = 1.702
norm_eps = 1e-06

def clamped_unit(gate_pre, up_pre):
    gated = jnp.minimum(gate_pre, clamp_limit)
    linear = jnp.clip(up_pre, -clamp_limit, clamp_limit)
    return (gated * jax.nn.sigmoid(sigmoid_slope * gated) * (linear + 1.0)).astype(jnp.bfloat16)

def rms_normed(tokens, norm_gain):
    values = tokens.astype(jnp.float32)
    inverse = lax.rsqrt(lax.optimization_barrier(jnp.mean(values * values, axis=-1, keepdims=True)) + norm_eps)
    return (values * inverse * norm_gain).astype(jnp.bfloat16)

def reference(tokens, norm_gain, routes, route_weight, expert_gate, expert_up, expert_down, dense_gate, dense_up, dense_down, gate_vector):
    normed = rms_normed(tokens, norm_gain)
    hidden = clamped_unit(jnp.dot(normed, dense_gate, preferred_element_type=jnp.float32), jnp.dot(normed, dense_up, preferred_element_type=jnp.float32))
    gate_logit = jnp.dot(hidden, gate_vector, preferred_element_type=jnp.float32)
    dense_out = jnp.dot(hidden, dense_down, preferred_element_type=jnp.float32)
    padded = jnp.concatenate([normed, jnp.zeros((1, D), jnp.bfloat16)], axis=0)
    half_width = F // N_TP

    def one_expert(totals, expert):
        matches = routes == expert
        chosen = jnp.any(matches, axis=1)
        weight = lax.optimization_barrier(jnp.sum(jnp.where(matches, route_weight, jnp.zeros_like(route_weight)), axis=1))
        weight = jnp.concatenate([weight, jnp.zeros((1,), weight.dtype)], axis=0)
        row_index = jnp.nonzero(chosen, size=N_EP * CAP, fill_value=TOKENS)[0].astype(jnp.int32)
        row_values = padded[row_index]
        expert_act = clamped_unit(jnp.dot(row_values, expert_gate[expert], preferred_element_type=jnp.float32), jnp.dot(row_values, expert_up[expert], preferred_element_type=jnp.float32))
        down_rows = expert_down[expert]
        outputs = jnp.zeros((row_values.shape[0], D), jnp.float32)
        for part_index in range(N_TP):
            pieces = jnp.dot(expert_act[:, part_index * half_width:(part_index + 1) * half_width], down_rows[part_index * half_width:(part_index + 1) * half_width], preferred_element_type=jnp.float32)
            outputs = outputs + lax.optimization_barrier(pieces.astype(jnp.bfloat16)).astype(jnp.float32)
        outputs = lax.optimization_barrier(outputs.astype(jnp.bfloat16)).astype(jnp.float32)
        totals = totals.at[row_index].add(weight[row_index][:, None] * outputs)
        return (totals, None)
    totals, _ = lax.scan(one_expert, jnp.zeros((TOKENS + 1, D), jnp.float32), jnp.arange(EXPERTS, dtype=jnp.int32))
    expert_mix = totals[:TOKENS]
    mixed = jax.nn.sigmoid(gate_logit)[:, None] * dense_out + expert_mix
    return mixed.astype(jnp.bfloat16)
```

```python
import math

import jax
import jax.numpy as jnp
from jax import lax
from jax.sharding import Mesh
from jax.sharding import PartitionSpec as P

EP = ("ep_0", "ep_1")
GRP_EP = ("grp", "ep_0", "ep_1")
EP_TP = ("ep_0", "ep_1", "tp")

clamp_limit = 7.0
sigmoid_slope = 1.702
norm_eps = 1e-06
capacity = 2
block = 2
lane = 128


def clamped_unit(gate_pre, up_pre):
    gated = jnp.minimum(gate_pre, clamp_limit)
    linear = jnp.clip(up_pre, -clamp_limit, clamp_limit)
    return (gated * jax.nn.sigmoid(sigmoid_slope * gated) * (linear + 1.0)).astype(jnp.bfloat16)


def rms_normed(tokens, norm_gain):
    values = tokens.astype(jnp.float32)
    inverse = lax.rsqrt(jnp.mean(values * values, axis=-1, keepdims=True) + norm_eps)
    return (values * inverse * norm_gain).astype(jnp.bfloat16)


def swap_cores(value):
    return lax.ppermute(value, "tp", [(0, 1), (1, 0)])


def from_block(value, down, across):
    high, wide = lax.axis_size("ep_0"), lax.axis_size("ep_1")
    pairs = [
        (y * wide + x, (y ^ down) * wide + (x ^ across)) for y in range(high) for x in range(wide)
    ]
    return lax.ppermute(value, EP, pairs)


def f32_dot(a, b, dims=(((1,), (0,)), ((), ()))):
    return lax.dot_general(a, b, dims, preferred_element_type=jnp.float32)


NT = (((1,), (1,)), ((), ()))


def per_device(
    tokens,
    norm_gain,
    routes,
    route_weight,
    expert_gate,
    expert_up,
    expert_down,
    dense_gate,
    dense_up,
    dense_down,
    gate_vector,
):
    tok_dev, width = tokens.shape
    half = width // lax.axis_size("tp")
    ep_count = lax.axis_size(EP)
    classes = block * block
    share = tok_dev // classes
    chunk = capacity + share
    side = lax.axis_size("ep_1")
    core = lax.axis_index("tp")
    units = dense_down.shape[0]

    experts = jnp.arange(ep_count, dtype=jnp.int32)
    named = routes[:, :, None] == experts[None, None, :]
    member = jnp.any(named, axis=1)
    weight = jnp.sum(jnp.where(named, route_weight[:, :, None], 0.0), axis=1)
    earlier = (
        jnp.arange(tok_dev)[:, None] > jnp.arange(tok_dev)[None, :]
    )
    rank = jnp.sum(jnp.where(earlier[:, :, None] & member[None, :, :], 1, 0), axis=1)
    slots = [member & (rank == r) for r in range(capacity)]
    klass = (experts // side % block) * block + experts % block
    rows = jnp.arange(tok_dev, dtype=jnp.int32)[:, None]
    shares = [rows == (klass * share + i)[None, :] for i in range(share)]
    places = jnp.stack(slots + shares, axis=-1)

    normed = rms_normed(tokens, norm_gain)
    mine = lax.dynamic_slice_in_dim(normed, core * half, half, 1)
    picked = places.astype(jnp.bfloat16).reshape(tok_dev, ep_count * chunk)
    outgoing = f32_dot(picked, mine, (((0,), (0,)), ((), ()))).astype(jnp.bfloat16)
    arrived = lax.all_to_all(
        outgoing.reshape(ep_count, chunk, half), EP, split_axis=0, concat_axis=0, tiled=True
    )
    down_mine = lax.dynamic_slice_in_dim(dense_down, core * half, half, 1)
    down_other = swap_cores(lax.dynamic_slice_in_dim(dense_down, (1 - core) * half, half, 1))
    vector = jnp.pad(gate_vector[:, None], ((0, 0), (0, lane - 1)))
    vector_other = swap_cores(vector)
    pack = jnp.concatenate(
        [dense_gate.T, dense_up.T, down_mine, vector, down_other, vector_other], axis=1
    )
    packs = [pack] + [from_block(pack, d, a) for d, a in ((0, 1), (1, 0), (1, 1))]
    packs = jnp.concatenate(packs, axis=0)
    gates = packs[:, :width]
    ups = packs[:, width : 2 * width]
    downs_mine = packs[:, 2 * width : 2 * width + half + lane]
    downs_other = packs[:, 2 * width + half + lane :]

    other = swap_cores(arrived)
    low = jnp.where(core == 0, arrived, other)
    high = jnp.where(core == 0, other, arrived)
    full = jnp.concatenate([low, high], axis=2)
    expert_rows = full[:, :capacity].reshape(ep_count * capacity, width)
    dense_rows = full[:, capacity:].reshape(ep_count * share, width)

    expert_act = clamped_unit(
        f32_dot(expert_rows, expert_gate[0]), f32_dot(expert_rows, expert_up[0])
    )
    partial_value = f32_dot(expert_act, expert_down[0]).astype(jnp.bfloat16)
    away = swap_cores(lax.dynamic_slice_in_dim(partial_value, (1 - core) * half, half, 1))
    here = lax.dynamic_slice_in_dim(partial_value, core * half, half, 1)
    expert_out = (here.astype(jnp.float32) + away.astype(jnp.float32)).astype(jnp.bfloat16)

    hidden = clamped_unit(f32_dot(dense_rows, gates, NT), f32_dot(dense_rows, ups, NT))
    hidden_other = swap_cores(hidden)
    terms = f32_dot(hidden, downs_mine) + f32_dot(hidden_other, downs_other)
    terms = terms.astype(jnp.bfloat16).reshape(ep_count, share, half + lane)
    expert_out = jnp.pad(
        expert_out.reshape(ep_count, capacity, half), ((0, 0), (0, 0), (0, lane))
    )
    returned = lax.all_to_all(
        jnp.concatenate([expert_out, terms], axis=1), EP, split_axis=0, concat_axis=0, tiled=True
    )
    shares = jnp.stack(shares, axis=-1)
    logits = returned[:, capacity:, half].astype(jnp.float32)
    gate_logit = jnp.sum(jnp.where(shares, logits[None], 0.0), axis=(1, 2))
    gate = jax.nn.sigmoid(gate_logit)[:, None, None]
    slot_weight = jnp.stack([jnp.where(s, weight, 0.0) for s in slots], axis=-1)
    mixing = jnp.concatenate([slot_weight, jnp.where(shares, gate, 0.0)], axis=-1)
    mixed = jnp.dot(
        mixing.reshape(tok_dev, -1),
        returned[:, :, :half].reshape(-1, half).astype(jnp.float32),
        precision=lax.Precision.HIGHEST,
    )
    return mixed.astype(jnp.bfloat16)


def solution(mesh):
    side = math.isqrt(mesh.shape["ep"])
    split = Mesh(
        mesh.devices.reshape(mesh.shape["grp"], side, side, mesh.shape["tp"]),
        ("grp", "ep_0", "ep_1", "tp"),
    )
    placed = (
        P(GRP_EP, None),
        P(),
        P(GRP_EP, None),
        P(GRP_EP, None),
        P(EP, None, "tp"),
        P(EP, None, "tp"),
        P(EP, "tp", None),
        P(None, EP_TP),
        P(None, EP_TP),
        P(EP_TP, None),
        P(EP_TP),
    )
    return jax.shard_map(
        per_device, mesh=split, in_specs=placed, out_specs=P(GRP_EP, "tp"), check_vma=False
    )
```

```python
import functools
import math

import jax
import jax.numpy as jnp
from jax import lax
from jax.experimental import pallas as pl
from jax.experimental.pallas import tpu as pltpu
from jax.sharding import Mesh
from jax.sharding import PartitionSpec as P

EP = ("ep_0", "ep_1")
GRP_EP = ("grp", "ep_0", "ep_1")
EP_TP = ("ep_0", "ep_1", "tp")

clamp_limit = 7.0
sigmoid_slope = 1.702
norm_eps = 1e-06
capacity = 2
lane = 128
shape = ((0, 0), (0, 1), (0, -1), (1, 0))
classes = len(shape)

F32, BF16, I32 = jnp.float32, jnp.bfloat16, jnp.int32


def clamped_unit(gate_pre, up_pre):
    gated = jnp.minimum(gate_pre, clamp_limit)
    linear = jnp.clip(up_pre, -clamp_limit, clamp_limit)
    return (gated * jax.nn.sigmoid(sigmoid_slope * gated) * (linear + 1.0)).astype(BF16)


def dot(a, b):
    return lax.dot_general(a, b, (((1,), (0,)), ((), ())), preferred_element_type=F32)


def dot_nt(a, b):
    return lax.dot_general(a, b, (((1,), (1,)), ((), ())), preferred_element_type=F32)


def iota(dims, dim):
    return lax.broadcasted_iota(I32, dims, dim)


def swap_cores(value):
    return lax.ppermute(value, "tp", [(0, 1), (1, 0)])


def from_chip(value, down, across):
    high, wide = lax.axis_size("ep_0"), lax.axis_size("ep_1")
    pairs = [
        ((y + down) % high * wide + (x + across) % wide, y * wide + x)
        for y in range(high)
        for x in range(wide)
    ]
    return lax.ppermute(value, EP, pairs)


def class_of(chip, wide):
    return (chip % wide + 2 * (chip // wide)) % classes


def dispatch_kernel(wide, core, tokens, gain, routes, out):
    tok_dev, width = tokens.shape
    half = width // 2
    top = routes.shape[0]
    slots = out.shape[0]
    values = tokens[...].astype(F32)
    inverse = lax.rsqrt(jnp.mean(values * values, axis=-1, keepdims=True) + norm_eps)
    low = core[0] == 0
    mine = jnp.where(low, values[:, :half], values[:, half:])
    scale = jnp.where(low, gain[:, :half], gain[:, half:])
    normed = (mine * inverse * scale).astype(BF16)
    slot = iota((slots, tok_dev), 0)
    row = iota((slots, tok_dev), 1)
    expert = slot // capacity
    member = jnp.zeros((slots, tok_dev), jnp.bool_)
    for k in range(top):
        member = member | (routes[k : k + 1, :] == expert)
    member = member.astype(F32)
    earlier = (iota((tok_dev, tok_dev), 0) < iota((tok_dev, tok_dev), 1)).astype(F32)
    rank = dot(member.astype(BF16), earlier.astype(BF16))
    taken = jnp.where(rank == (slot % capacity).astype(F32), member, 0.0)
    share = tok_dev // classes
    wanted = (row == class_of(expert, wide) * share + slot % capacity).astype(F32)
    out[:, :half] = dot(taken.astype(BF16), normed).astype(BF16)
    out[:, half:] = dot(wanted.astype(BF16), normed).astype(BF16)


def pack_kernel(gate, up, down, vector, routes, weights, pack, combine):
    units, width = gate.shape
    top, tok_dev = routes.shape
    slots = combine.shape[1]
    pack[:, :width] = gate[...]
    pack[:, width : 2 * width] = up[...]
    pack[:, 2 * width : 3 * width] = down[...]
    same = iota((units, units), 0) == iota((units, units), 1)
    spread = jnp.where(same, vector[...].astype(F32), 0.0).astype(BF16)
    first = (iota((units, lane), 1) == 0).astype(F32).astype(BF16)
    pack[:, 3 * width :] = dot(spread, first).astype(BF16)
    slot = iota((tok_dev, slots), 1)
    eye = iota((tok_dev, tok_dev), 0) == iota((tok_dev, tok_dev), 1)
    member = jnp.zeros((tok_dev, slots), F32)
    weight = jnp.zeros((tok_dev, slots), F32)
    for k in range(top):
        named = jnp.sum(jnp.where(eye, routes[k : k + 1, :], 0), axis=1, keepdims=True)
        worth = jnp.sum(jnp.where(eye, weights[k : k + 1, :], 0.0), axis=1, keepdims=True)
        hit = named == slot // capacity
        member = jnp.where(hit, 1.0, member)
        weight = jnp.where(hit, worth, weight)
    earlier = (iota((tok_dev, tok_dev), 1) < iota((tok_dev, tok_dev), 0)).astype(F32)
    rank = dot(earlier.astype(BF16), member.astype(BF16))
    combine[...] = jnp.where(rank == (slot % capacity).astype(F32), weight, 0.0)


def expert_kernel(core, mine, other, gate, up, down, here, away):
    half = mine.shape[1] // 2
    at = pl.multiple_of(core[0] * half, half)
    to = pl.multiple_of((1 - core[0]) * half, half)
    x = mine[:, :half]
    y = other[:, :half]
    gate_pre = dot(x, gate[0, pl.ds(at, half), :]) + dot(y, gate[0, pl.ds(to, half), :])
    up_pre = dot(x, up[0, pl.ds(at, half), :]) + dot(y, up[0, pl.ds(to, half), :])
    act = clamped_unit(gate_pre, up_pre)
    away[...] = dot(act, down[0, :, pl.ds(to, half)]).astype(BF16)
    here[...] = dot(act, down[0, :, pl.ds(at, half)]).astype(BF16)


def dense_kernel(core, mine, other, *refs):
    packs, (here, away) = refs[:classes], refs[classes:]
    half = mine.shape[1] // 2
    width = 2 * half
    at = pl.multiple_of(core[0] * half, half)
    to = pl.multiple_of((1 - core[0]) * half, half)
    x = mine[:, half:]
    y = other[:, half:]

    def rows(start, size):
        return jnp.concatenate([p[:, pl.ds(start, size)] for p in packs], axis=0)

    gate_pre = dot_nt(x, rows(at, half)) + dot_nt(y, rows(to, half))
    up_pre = dot_nt(x, rows(width + at, half)) + dot_nt(y, rows(width + to, half))
    hidden = clamped_unit(gate_pre, up_pre)
    logit = dot(hidden, rows(3 * width, lane)).astype(BF16)
    away[:, :half] = dot(hidden, rows(2 * width + to, half)).astype(BF16)
    away[:, half:] = logit
    here[:, :half] = dot(hidden, rows(2 * width + at, half)).astype(BF16)
    here[:, half:] = logit


def join_kernel(expert_here, expert_away, dense_here, dense_away, out):
    half = expert_here.shape[1]
    out[:, :half] = (expert_here[...].astype(F32) + expert_away[...].astype(F32)).astype(BF16)
    out[:, half:] = (dense_here[...].astype(F32) + dense_away[...].astype(F32)).astype(BF16)


def mix_kernel(wide, returned, combine, out):
    tok_dev, half = out.shape
    slots = returned.shape[0]
    slot = iota((tok_dev, slots), 1)
    share = tok_dev // classes
    owner = class_of(slot // capacity, wide) * share + slot % capacity
    wanted = (iota((tok_dev, slots), 0) == owner).astype(F32).astype(BF16)
    dense_out = dot(wanted, returned[:, half : 2 * half])
    gate_logit = dot(wanted, returned[:, 2 * half :])[:, :1]
    first = combine[...].astype(BF16)
    rest = combine[...] - first.astype(F32)
    second = rest.astype(BF16)
    third = (rest - second.astype(F32)).astype(BF16)
    rows = returned[:, :half]
    expert_mix = dot(first, rows) + (dot(second, rows) + dot(third, rows))
    out[...] = (jax.nn.sigmoid(gate_logit) * dense_out + expert_mix).astype(BF16)


def call(kernel, outs, *operands):
    specs = [pl.BlockSpec(memory_space=pltpu.VMEM) for _ in operands]
    if operands[0].dtype == I32 and operands[0].ndim == 1:
        specs[0] = pl.BlockSpec(memory_space=pltpu.SMEM)
    many = isinstance(outs, list)
    spec = pl.BlockSpec(memory_space=pltpu.VMEM)
    return pl.pallas_call(
        kernel,
        out_shape=outs,
        in_specs=specs,
        out_specs=[spec] * len(outs) if many else spec,
    )(*operands)


def per_device(
    tokens,
    norm_gain,
    routes,
    route_weight,
    expert_gate,
    expert_up,
    expert_down,
    dense_gate,
    dense_up,
    dense_down,
    gate_vector,
):
    tok_dev, width = tokens.shape
    half = width // lax.axis_size("tp")
    ep_count = lax.axis_size(EP)
    wide = lax.axis_size("ep_1")
    slots = ep_count * capacity
    units = dense_down.shape[0]
    core = lax.axis_index("tp").reshape(1)

    def exchange(rows):
        return lax.all_to_all(
            rows.reshape(ep_count, capacity, -1), EP, split_axis=0, concat_axis=0, tiled=True
        )

    def out(*dims, dtype=BF16):
        return jax.ShapeDtypeStruct(dims, dtype)

    outgoing = call(
        functools.partial(dispatch_kernel, wide),
        out(slots, width),
        core,
        tokens,
        norm_gain.reshape(1, -1),
        routes.T,
    )
    arrived = exchange(outgoing)
    pack, combine = call(
        pack_kernel,
        [out(units, 3 * width + lane), out(tok_dev, slots, dtype=F32)],
        dense_gate.T,
        dense_up.T,
        dense_down,
        gate_vector.reshape(1, -1),
        routes.T,
        route_weight.T,
    )
    packs = [pack] + [from_chip(pack, *offset) for offset in shape[1:]]
    other = swap_cores(arrived).reshape(slots, width)
    mine = arrived.reshape(slots, width)
    expert_here, expert_away = call(
        expert_kernel,
        [out(slots, half), out(slots, half)],
        core,
        mine,
        other,
        expert_gate,
        expert_up,
        expert_down,
    )
    expert_away = swap_cores(expert_away)
    dense_here, dense_away = call(
        dense_kernel,
        [out(slots, half + lane), out(slots, half + lane)],
        core,
        mine,
        other,
        *packs,
    )
    dense_away = swap_cores(dense_away)
    terms = call(
        join_kernel,
        out(slots, width + lane),
        expert_here,
        expert_away,
        dense_here,
        dense_away,
    )
    returned = exchange(terms).reshape(slots, width + lane)
    return call(functools.partial(mix_kernel, wide), out(tok_dev, half), returned, combine)


def solution(mesh):
    side = math.isqrt(mesh.shape["ep"])
    split = Mesh(
        mesh.devices.reshape(mesh.shape["grp"], side, side, mesh.shape["tp"]),
        ("grp", "ep_0", "ep_1", "tp"),
    )
    placed = (
        P(GRP_EP, None),
        P(),
        P(GRP_EP, None),
        P(GRP_EP, None),
        P(EP, None, "tp"),
        P(EP, None, "tp"),
        P(EP, "tp", None),
        P(None, EP_TP),
        P(None, EP_TP),
        P(EP_TP, None),
        P(EP_TP),
    )
    return jax.shard_map(
        per_device, mesh=split, in_specs=placed, out_specs=P(GRP_EP, "tp"), check_vma=False
    )
```

```python
import functools
import math

import jax
import jax.numpy as jnp
from jax import lax
from jax.experimental import pallas as pl
from jax.experimental.pallas import tpu as pltpu
from jax.sharding import Mesh
from jax.sharding import PartitionSpec as P


EP = ("ep_0", "ep_1")
GRP_EP = ("grp", "ep_0", "ep_1")
EP_TP = ("ep_0", "ep_1", "tp")

clamp_limit = 7.0
sigmoid_slope = 1.702
norm_eps = 1e-06
capacity = 2
lane = 128
shape = ((0, 0), (0, 1), (0, -1), (1, 0))
classes = len(shape)

F32, BF16, I32 = jnp.float32, jnp.bfloat16, jnp.int32


def clamped_unit(gate_pre, up_pre):
    gated = jnp.minimum(gate_pre, clamp_limit)
    linear = jnp.clip(up_pre, -clamp_limit, clamp_limit)
    return (gated * jax.nn.sigmoid(sigmoid_slope * gated) * (linear + 1.0)).astype(BF16)


def dot(a, b):
    return lax.dot_general(a, b, (((1,), (0,)), ((), ())), preferred_element_type=F32)


def dot_nt(a, b):
    return lax.dot_general(a, b, (((1,), (1,)), ((), ())), preferred_element_type=F32)


def iota(dims, dim):
    return lax.broadcasted_iota(I32, dims, dim)


def swap_cores(value):
    return lax.ppermute(value, "tp", [(0, 1), (1, 0)])


def from_chip(value, down, across):
    high, wide = lax.axis_size("ep_0"), lax.axis_size("ep_1")
    pairs = [
        ((y + down) % high * wide + (x + across) % wide, y * wide + x)
        for y in range(high)
        for x in range(wide)
    ]
    return lax.ppermute(value, EP, pairs)


def class_of(chip, wide):
    return (chip % wide + 2 * (chip // wide)) % classes


def dispatch_kernel(wide, core, tokens_hbm, gain_hbm, routes_hbm, out, tokens, gain, routes, sems):
    copies = [
        pltpu.make_async_copy(src, dst, sems.at[n])
        for n, (src, dst) in enumerate(
            ((tokens_hbm, tokens), (routes_hbm, routes), (gain_hbm, gain))
        )
    ]
    for copy in copies:
        copy.start()
    tok_dev, width = tokens.shape
    half = width // 2
    top = routes.shape[0]
    ep_count = out.shape[0]
    slots = ep_count * capacity
    slot = iota((slots, tok_dev), 0)
    row = iota((slots, tok_dev), 1)
    expert = slot // capacity
    share = tok_dev // classes
    wanted = (row == class_of(expert, wide) * share + slot % capacity).astype(F32).astype(BF16)
    earlier = (iota((tok_dev, tok_dev), 0) < iota((tok_dev, tok_dev), 1)).astype(F32).astype(BF16)
    copies[1].wait()
    member = jnp.zeros((slots, tok_dev), F32)
    for k in range(top):
        member = jnp.where(routes[k : k + 1, :] == expert, 1.0, member)
    rank = dot(member.astype(BF16), earlier)
    taken = jnp.where(rank == (slot % capacity).astype(F32), member, 0.0).astype(BF16)
    copies[0].wait()
    copies[2].wait()
    values = tokens[...].astype(F32)
    inverse = lax.rsqrt(jnp.mean(values * values, axis=-1, keepdims=True) + norm_eps)
    low = core[0] == 0
    mine = jnp.where(low, values[:, :half], values[:, half:]) * inverse
    blocks = half // lane
    normed = []
    for n in range(blocks):
        scale = jnp.where(low, gain[n : n + 1, :], gain[blocks + n : blocks + n + 1, :])
        normed.append((mine[:, n * lane : (n + 1) * lane] * scale).astype(BF16))
    normed = jnp.concatenate(normed, axis=1)
    out[:, :, :half] = dot(taken, normed).astype(BF16).reshape(ep_count, capacity, half)
    out[:, :, half:] = dot(wanted, normed).astype(BF16).reshape(ep_count, capacity, half)


def pack_kernel(
    gate, up, down, vector_hbm, routes_hbm, weights_hbm, pack, combine, vector, routes, weights, sems
):
    units, width = gate.shape
    copies = [
        pltpu.make_async_copy(src, dst, sems.at[n])
        for n, (src, dst) in enumerate(
            (
                (vector_hbm, vector),
                (routes_hbm, routes),
                (weights_hbm, weights),
                (gate, pack.at[:, :width]),
                (up, pack.at[:, width : 2 * width]),
                (down, pack.at[:, 2 * width : 3 * width]),
            )
        )
    ]
    for copy in copies:
        copy.start()
    top, tok_dev = routes.shape
    slots = combine.shape[1]
    same = iota((units, units), 0) == iota((units, units), 1)
    first = (iota((units, lane), 1) == 0).astype(F32).astype(BF16)
    slot = iota((tok_dev, slots), 1)
    eye = iota((tok_dev, tok_dev), 0) == iota((tok_dev, tok_dev), 1)
    earlier = (iota((tok_dev, tok_dev), 1) < iota((tok_dev, tok_dev), 0)).astype(F32).astype(BF16)
    for copy in copies[:3]:
        copy.wait()
    spread = jnp.where(same, vector[...].astype(F32), 0.0).astype(BF16)
    pack[:, 3 * width :] = dot(spread, first).astype(BF16)
    member = jnp.zeros((tok_dev, slots), F32)
    weight = jnp.zeros((tok_dev, slots), F32)
    for k in range(top):
        named = jnp.sum(jnp.where(eye, routes[k : k + 1, :], 0), axis=1, keepdims=True)
        worth = jnp.sum(jnp.where(eye, weights[k : k + 1, :], 0.0), axis=1, keepdims=True)
        hit = named == slot // capacity
        member = jnp.where(hit, 1.0, member)
        weight = jnp.where(hit, worth, weight)
    rank = dot(earlier, member.astype(BF16))
    combine[...] = jnp.where(rank == (slot % capacity).astype(F32), weight, 0.0)
    for copy in copies[3:]:
        copy.wait()


def copy_all(pairs, sems):
    copies = [pltpu.make_async_copy(src, dst, sems.at[n]) for n, (src, dst) in enumerate(pairs)]
    for copy in copies:
        copy.start()
    return copies


def halves(core, half):
    at = pl.multiple_of(core[0] * half, half)
    to = pl.multiple_of((1 - core[0]) * half, half)
    return at, to


def fetch_kernel(core, gate_hbm, up_hbm, gate, up, sems):
    half = gate.shape[0]
    at, _ = halves(core, half)
    pairs = [(src.at[0, pl.ds(at, half), :], dst) for src, dst in ((gate_hbm, gate), (up_hbm, up))]
    for copy in copy_all(pairs, sems):
        copy.wait()


def own_kernel(
    core, mine, gate, up, gate_hbm, up_hbm, down_hbm, gate_pre, up_pre, gate_to, up_to, down, sems
):
    half = gate.shape[0]
    _, to = halves(core, half)
    copies = copy_all(
        (
            (gate_hbm.at[0, pl.ds(to, half), :], gate_to),
            (up_hbm.at[0, pl.ds(to, half), :], up_to),
            (down_hbm.at[0], down),
        ),
        sems,
    )
    x = mine[:, :, :half].reshape(-1, half)
    gate_pre[...] = dot(x, gate[...])
    up_pre[...] = dot(x, up[...])
    for copy in copies:
        copy.wait()


def rest_kernel(core, other, gate_pre, up_pre, gate, up, down, *refs):
    packs_hbm, (act, away, packs, sems) = refs[: classes - 1], refs[classes - 1 :]
    units = packs_hbm[0].shape[0]
    copies = copy_all(
        [(src, packs.at[n * units : (n + 1) * units, :]) for n, src in enumerate(packs_hbm)], sems
    )
    half = gate.shape[0]
    _, to = halves(core, half)
    y = other[:, :, :half].reshape(-1, half)
    value = clamped_unit(gate_pre[...] + dot(y, gate[...]), up_pre[...] + dot(y, up[...]))
    act[...] = value
    away[...] = dot(value, down[:, pl.ds(to, half)]).astype(BF16)
    for copy in copies:
        copy.wait()


def rows(packs, start, size):
    return jnp.concatenate([p[:, pl.ds(start, size)] for p in packs], axis=0)


def dense_kernel(core, mine, other, pack, neighbours, hidden, away):
    packs = (pack, neighbours)
    half = mine.shape[2] // 2
    width = 2 * half
    at, to = halves(core, half)
    x = mine[:, :, half:].reshape(-1, half)
    y = other[:, :, half:].reshape(-1, half)
    gate_pre = dot_nt(x, rows(packs, at, half)) + dot_nt(y, rows(packs, to, half))
    up_pre = dot_nt(x, rows(packs, width + at, half)) + dot_nt(y, rows(packs, width + to, half))
    value = clamped_unit(gate_pre, up_pre)
    hidden[...] = value
    away[:, :half] = dot(value, rows(packs, 2 * width + to, half)).astype(BF16)
    away[:, half:] = dot(value, rows(packs, 3 * width, lane)).astype(BF16)


def here_kernel(core, act, hidden, down, pack, neighbours, out):
    packs = (pack, neighbours)
    half = down.shape[1] // 2
    width = 2 * half
    at, _ = halves(core, half)
    out[:, :half] = dot(act[...], down[:, pl.ds(at, half)]).astype(BF16)
    value = hidden[...]
    out[:, half:width] = dot(value, rows(packs, 2 * width + at, half)).astype(BF16)
    out[:, width:] = dot(value, rows(packs, 3 * width, lane)).astype(BF16)


def join_kernel(here, expert_away, dense_away, out):
    half = expert_away.shape[1]
    shape3 = out.shape[:2] + (-1,)
    mine = here[...].astype(F32)
    expert = (mine[:, :half] + expert_away[...].astype(F32)).astype(BF16)
    dense = (mine[:, half:] + dense_away[...].astype(F32)).astype(BF16)
    out[:, :, :half] = expert.reshape(shape3)
    out[:, :, half:] = dense.reshape(shape3)


def mix_kernel(wide, returned, combine, out):
    tok_dev, half = out.shape
    slots = returned.shape[0] * returned.shape[1]
    slot = iota((tok_dev, slots), 1)
    share = tok_dev // classes
    owner = class_of(slot // capacity, wide) * share + slot % capacity
    wanted = (iota((tok_dev, slots), 0) == owner).astype(F32).astype(BF16)
    dense_out = dot(wanted, returned[:, :, half : 2 * half].reshape(slots, half))
    gate_logit = dot(wanted, returned[:, :, 2 * half :].reshape(slots, lane))[:, :1]
    first = combine[...].astype(BF16)
    rest = combine[...] - first.astype(F32)
    second = rest.astype(BF16)
    third = (rest - second.astype(F32)).astype(BF16)
    expert_rows = returned[:, :, :half].reshape(slots, half)
    expert_mix = dot(first, expert_rows) + (dot(second, expert_rows) + dot(third, expert_rows))
    out[...] = (jax.nn.sigmoid(gate_logit) * dense_out + expert_mix).astype(BF16)


def call(kernel, outs, *operands, inside=0, scratch=(), room=8 * 2**20):
    specs, placed = [], []
    for n, operand in enumerate(operands):
        if n >= len(operands) - inside:
            specs.append(pl.BlockSpec(memory_space=pl.ANY))
            placed.append(pltpu.with_memory_space_constraint(operand, pltpu.HBM))
        elif operand.dtype == I32 and operand.ndim == 1:
            specs.append(pl.BlockSpec(memory_space=pltpu.SMEM))
            placed.append(operand)
        else:
            specs.append(pl.BlockSpec(memory_space=pltpu.VMEM))
            placed.append(operand)
    many = isinstance(outs, list)
    spec = pl.BlockSpec(memory_space=pltpu.VMEM)
    return pl.pallas_call(
        kernel,
        out_shape=outs,
        in_specs=specs,
        out_specs=[spec] * len(outs) if many else spec,
        scratch_shapes=list(scratch),
        cost_estimate=pl.CostEstimate(flops=10**9, transcendentals=0, bytes_accessed=0),
        compiler_params=pltpu.CompilerParams(vmem_limit_bytes=room),
    )(*placed)


def per_device(
    tokens,
    norm_gain,
    routes,
    route_weight,
    expert_gate,
    expert_up,
    expert_down,
    dense_gate,
    dense_up,
    dense_down,
    gate_vector,
):
    tok_dev, width = tokens.shape
    top = routes.shape[1]
    half = width // lax.axis_size("tp")
    ep_count = lax.axis_size(EP)
    wide = lax.axis_size("ep_1")
    slots = ep_count * capacity
    units, hidden_units = dense_down.shape[0], expert_down.shape[1]
    core = lax.axis_index("tp").reshape(1)

    def exchange(rows):
        return lax.all_to_all(rows, EP, split_axis=0, concat_axis=0, tiled=True)

    def out(*dims, dtype=BF16):
        return pltpu.VMEM(dims, dtype)

    outgoing = call(
        functools.partial(dispatch_kernel, wide),
        out(ep_count, capacity, width),
        core,
        tokens,
        norm_gain.reshape(-1, lane),
        routes.T,
        inside=3,
        scratch=(
            pltpu.VMEM((tok_dev, width), BF16),
            pltpu.VMEM((width // lane, lane), F32),
            pltpu.VMEM((top, tok_dev), I32),
            pltpu.SemaphoreType.DMA((3,)),
        ),
    )
    mine = exchange(outgoing)
    pack, combine = call(
        pack_kernel,
        [out(units, 3 * width + lane), out(tok_dev, slots, dtype=F32)],
        dense_gate.T,
        dense_up.T,
        dense_down,
        gate_vector.reshape(1, -1),
        routes.T,
        route_weight.T,
        inside=6,
        scratch=(
            pltpu.VMEM((1, units), BF16),
            pltpu.VMEM((top, tok_dev), I32),
            pltpu.VMEM((top, tok_dev), F32),
            pltpu.SemaphoreType.DMA((6,)),
        ),
    )
    packs = []
    for offset in shape[1:]:
        packs.append(from_chip(pack, *offset))
    dma = pltpu.SemaphoreType.DMA
    gate, up = call(
        fetch_kernel,
        [out(half, hidden_units)] * 2,
        core,
        expert_gate,
        expert_up,
        inside=2,
        scratch=(dma((2,)),),
    )
    other = swap_cores(mine)
    gate_pre, up_pre, gate, up, down = call(
        own_kernel,
        [out(slots, hidden_units, dtype=F32)] * 2
        + [out(half, hidden_units)] * 2
        + [out(hidden_units, width)],
        core,
        mine,
        gate,
        up,
        expert_gate,
        expert_up,
        expert_down,
        inside=3,
        scratch=(dma((3,)),),
    )
    act, expert_away, neighbours = call(
        rest_kernel,
        [out(slots, hidden_units), out(slots, half), out((classes - 1) * units, 3 * width + lane)],
        core,
        other,
        gate_pre,
        up_pre,
        gate,
        up,
        down,
        *packs,
        inside=classes - 1,
        scratch=(dma((classes - 1,)),),
    )
    expert_away = swap_cores(expert_away)
    hidden, dense_away = call(
        dense_kernel,
        [out(slots, classes * units), out(slots, half + lane)],
        core,
        mine,
        other,
        pack,
        neighbours,
    )
    dense_away = swap_cores(dense_away)
    here = call(here_kernel, out(slots, width + lane), core, act, hidden, down, pack, neighbours)
    terms = call(join_kernel, out(ep_count, capacity, width + lane), here, expert_away, dense_away)
    returned = exchange(terms)
    return call(
        functools.partial(mix_kernel, wide),
        jax.ShapeDtypeStruct((tok_dev, half), BF16),
        returned,
        combine,
    )


def solution(mesh):
    side = math.isqrt(mesh.shape["ep"])
    split = Mesh(
        mesh.devices.reshape(mesh.shape["grp"], side, side, mesh.shape["tp"]),
        ("grp", "ep_0", "ep_1", "tp"),
    )
    placed = (
        P(GRP_EP, None),
        P(),
        P(GRP_EP, None),
        P(GRP_EP, None),
        P(EP, None, "tp"),
        P(EP, None, "tp"),
        P(EP, "tp", None),
        P(None, EP_TP),
        P(None, EP_TP),
        P(EP_TP, None),
        P(EP_TP),
    )

    return jax.shard_map(
        per_device, mesh=split, in_specs=placed, out_specs=P(GRP_EP, "tp"), check_vma=False
    )
```

```python
import functools
import math

import jax
import jax.numpy as jnp
from jax import lax
from jax.experimental import pallas as pl
from jax.experimental.pallas import tpu as pltpu
from jax.sharding import Mesh
from jax.sharding import PartitionSpec as P


EP = ("ep_0", "ep_1")
GRP_EP = ("grp", "ep_0", "ep_1")
EP_TP = ("ep_0", "ep_1", "tp")

clamp_limit = 7.0
sigmoid_slope = 1.702
norm_eps = 1e-06
capacity = 2
lane = 128
shape = ((0, 0), (0, 1), (0, -1), (1, 0))
classes = len(shape)

F32, BF16, I32 = jnp.float32, jnp.bfloat16, jnp.int32


def clamped_unit(gate_pre, up_pre):
    gated = jnp.minimum(gate_pre, clamp_limit)
    linear = jnp.clip(up_pre, -clamp_limit, clamp_limit)
    return (gated * jax.nn.sigmoid(sigmoid_slope * gated) * (linear + 1.0)).astype(BF16)


def dot(a, b):
    return lax.dot_general(a, b, (((1,), (0,)), ((), ())), preferred_element_type=F32)


def dot_nt(a, b):
    return lax.dot_general(a, b, (((1,), (1,)), ((), ())), preferred_element_type=F32)


def iota(dims, dim):
    return lax.broadcasted_iota(I32, dims, dim)


def swap_cores(value):
    return lax.ppermute(value, "tp", [(0, 1), (1, 0)])


def from_chip(value, down, across):
    high, wide = lax.axis_size("ep_0"), lax.axis_size("ep_1")
    pairs = [
        ((y + down) % high * wide + (x + across) % wide, y * wide + x)
        for y in range(high)
        for x in range(wide)
    ]
    return lax.ppermute(value, EP, pairs)


def class_of(chip, wide):
    return (chip % wide + 2 * (chip // wide)) % classes


def copy_all(pairs, sems):
    copies = [pltpu.make_async_copy(src, dst, sems.at[n]) for n, (src, dst) in enumerate(pairs)]
    for copy in copies:
        copy.start()
    return copies


def first_kernel(
    wide,
    core,
    tokens_hbm,
    routes_hbm,
    gain_hbm,
    vector_hbm,
    gate_hbm,
    up_hbm,
    down_hbm,
    out,
    pack,
    tokens,
    routes,
    gain,
    vector,
    sems,
):
    tok_dev, width = tokens.shape
    copies = copy_all(
        (
            (routes_hbm, routes),
            (tokens_hbm, tokens),
            (gain_hbm, gain),
            (vector_hbm, vector),
            (gate_hbm, pack.at[:, :width]),
            (up_hbm, pack.at[:, width : 2 * width]),
            (down_hbm, pack.at[:, 2 * width : 3 * width]),
        ),
        sems,
    )
    half = width // 2
    top = routes.shape[0]
    ep_count = out.shape[0]
    slots = ep_count * capacity
    units = pack.shape[0]
    slot = iota((slots, tok_dev), 0)
    row = iota((slots, tok_dev), 1)
    expert = slot // capacity
    share = tok_dev // classes
    wanted = (row == class_of(expert, wide) * share + slot % capacity).astype(F32).astype(BF16)
    earlier = (iota((tok_dev, tok_dev), 0) < iota((tok_dev, tok_dev), 1)).astype(F32).astype(BF16)
    same = iota((units, units), 0) == iota((units, units), 1)
    lead = (iota((units, lane), 1) == 0).astype(F32).astype(BF16)
    copies[0].wait()
    member = jnp.zeros((slots, tok_dev), F32)
    for k in range(top):
        member = jnp.where(routes[k : k + 1, :] == expert, 1.0, member)
    rank = dot(member.astype(BF16), earlier)
    taken = jnp.where(rank == (slot % capacity).astype(F32), member, 0.0).astype(BF16)
    for copy in copies[1:4]:
        copy.wait()
    values = tokens[...].astype(F32)
    inverse = lax.rsqrt(jnp.mean(values * values, axis=-1, keepdims=True) + norm_eps)
    low = core[0] == 0
    mine = jnp.where(low, values[:, :half], values[:, half:]) * inverse
    blocks = half // lane
    normed = []
    for n in range(blocks):
        scale = jnp.where(low, gain[n : n + 1, :], gain[blocks + n : blocks + n + 1, :])
        normed.append((mine[:, n * lane : (n + 1) * lane] * scale).astype(BF16))
    normed = jnp.concatenate(normed, axis=1)
    spread = jnp.where(same, vector[...].astype(F32), 0.0).astype(BF16)
    pack[:, 3 * width :] = dot(spread, lead).astype(BF16)
    out[:, :, :half] = dot(taken, normed).astype(BF16).reshape(ep_count, capacity, half)
    out[:, :, half:] = dot(wanted, normed).astype(BF16).reshape(ep_count, capacity, half)
    for copy in copies[4:]:
        copy.wait()


def weigh(routes, weights, combine):
    top, tok_dev = routes.shape
    slots = combine.shape[1]
    slot = iota((tok_dev, slots), 1)
    eye = iota((tok_dev, tok_dev), 0) == iota((tok_dev, tok_dev), 1)
    earlier = (iota((tok_dev, tok_dev), 1) < iota((tok_dev, tok_dev), 0)).astype(F32).astype(BF16)
    member = jnp.zeros((tok_dev, slots), F32)
    weight = jnp.zeros((tok_dev, slots), F32)
    for k in range(top):
        named = jnp.sum(jnp.where(eye, routes[k : k + 1, :], 0), axis=1, keepdims=True)
        worth = jnp.sum(jnp.where(eye, weights[k : k + 1, :], 0.0), axis=1, keepdims=True)
        hit = named == slot // capacity
        member = jnp.where(hit, 1.0, member)
        weight = jnp.where(hit, worth, weight)
    rank = dot(earlier, member.astype(BF16))
    combine[...] = jnp.where(rank == (slot % capacity).astype(F32), weight, 0.0)


def halves(core, half):
    at = pl.multiple_of(core[0] * half, half)
    to = pl.multiple_of((1 - core[0]) * half, half)
    return at, to


def own_kernel(
    core,
    mine,
    gate,
    up_hbm,
    routes_hbm,
    weights_hbm,
    gate_pre,
    up_pre,
    up,
    combine,
    routes,
    weights,
    sems,
):
    half = mine.shape[2] // 2
    at, to = halves(core, half)
    copies = copy_all(
        (
            (up_hbm.at[0, pl.ds(at, half), :], up.at[pl.ds(at, half), :]),
            (routes_hbm, routes),
            (weights_hbm, weights),
            (up_hbm.at[0, pl.ds(to, half), :], up.at[pl.ds(to, half), :]),
        ),
        sems,
    )
    x = mine[:, :, :half].reshape(-1, half)
    gate_pre[...] = dot(x, gate[0, pl.ds(at, half), :])
    copies[1].wait()
    copies[2].wait()
    weigh(routes, weights, combine)
    copies[0].wait()
    up_pre[...] = dot(x, up[pl.ds(at, half), :])
    copies[3].wait()


def rest_kernel(core, other, gate_pre, up_pre, gate, up, down, act, away):
    half = other.shape[2] // 2
    _, to = halves(core, half)
    y = other[:, :, :half].reshape(-1, half)
    value = clamped_unit(
        gate_pre[...] + dot(y, gate[0, pl.ds(to, half), :]),
        up_pre[...] + dot(y, up[pl.ds(to, half), :]),
    )
    act[...] = value
    away[...] = dot(value, down[0, :, pl.ds(to, half)]).astype(BF16)


def rows(packs, start, size):
    return jnp.concatenate([p[:, pl.ds(start, size)] for p in packs], axis=0)


def dense_kernel(core, mine, other, *refs):
    packs, (hidden, away) = refs[:classes], refs[classes:]
    half = mine.shape[2] // 2
    width = 2 * half
    at, to = halves(core, half)
    x = mine[:, :, half:].reshape(-1, half)
    y = other[:, :, half:].reshape(-1, half)
    gate_pre = dot_nt(x, rows(packs, at, half)) + dot_nt(y, rows(packs, to, half))
    up_pre = dot_nt(x, rows(packs, width + at, half)) + dot_nt(y, rows(packs, width + to, half))
    value = clamped_unit(gate_pre, up_pre)
    hidden[...] = value
    away[:, :half] = dot(value, rows(packs, 2 * width + to, half)).astype(BF16)
    away[:, half:] = dot(value, rows(packs, 3 * width, lane)).astype(BF16)


def here_kernel(core, act, hidden, down, *refs):
    packs, out = refs[:classes], refs[classes]
    half = down.shape[2] // 2
    width = 2 * half
    at, _ = halves(core, half)
    out[:, :half] = dot(act[...], down[0, :, pl.ds(at, half)]).astype(BF16)
    value = hidden[...]
    out[:, half:width] = dot(value, rows(packs, 2 * width + at, half)).astype(BF16)
    out[:, width:] = dot(value, rows(packs, 3 * width, lane)).astype(BF16)


def join_kernel(here, expert_away, dense_away, out):
    half = expert_away.shape[1]
    shape3 = out.shape[:2] + (-1,)
    mine = here[...].astype(F32)
    expert = (mine[:, :half] + expert_away[...].astype(F32)).astype(BF16)
    dense = (mine[:, half:] + dense_away[...].astype(F32)).astype(BF16)
    out[:, :, :half] = expert.reshape(shape3)
    out[:, :, half:] = dense.reshape(shape3)


def mix_kernel(wide, returned, combine, out):
    tok_dev, half = out.shape
    slots = returned.shape[0] * returned.shape[1]
    slot = iota((tok_dev, slots), 1)
    share = tok_dev // classes
    owner = class_of(slot // capacity, wide) * share + slot % capacity
    wanted = (iota((tok_dev, slots), 0) == owner).astype(F32).astype(BF16)
    dense_out = dot(wanted, returned[:, :, half : 2 * half].reshape(slots, half))
    gate_logit = dot(wanted, returned[:, :, 2 * half :].reshape(slots, lane))[:, :1]
    first = combine[...].astype(BF16)
    rest = combine[...] - first.astype(F32)
    second = rest.astype(BF16)
    third = (rest - second.astype(F32)).astype(BF16)
    expert_rows = returned[:, :, :half].reshape(slots, half)
    expert_mix = dot(first, expert_rows) + (dot(second, expert_rows) + dot(third, expert_rows))
    out[...] = (jax.nn.sigmoid(gate_logit) * dense_out + expert_mix).astype(BF16)


def call(kernel, outs, *operands, inside=0, scratch=(), room=8 * 2**20):
    specs, placed = [], []
    for n, operand in enumerate(operands):
        if n >= len(operands) - inside:
            specs.append(pl.BlockSpec(memory_space=pl.ANY))
            placed.append(pltpu.with_memory_space_constraint(operand, pltpu.HBM))
        elif operand.dtype == I32 and operand.ndim == 1:
            specs.append(pl.BlockSpec(memory_space=pltpu.SMEM))
            placed.append(operand)
        else:
            specs.append(pl.BlockSpec(memory_space=pltpu.VMEM))
            placed.append(operand)
    many = isinstance(outs, list)
    spec = pl.BlockSpec(memory_space=pltpu.VMEM)
    return pl.pallas_call(
        kernel,
        out_shape=outs,
        in_specs=specs,
        out_specs=[spec] * len(outs) if many else spec,
        scratch_shapes=list(scratch),
        cost_estimate=pl.CostEstimate(flops=10**9, transcendentals=0, bytes_accessed=0),
        compiler_params=pltpu.CompilerParams(vmem_limit_bytes=room),
    )(*placed)


def per_device(
    tokens,
    norm_gain,
    routes,
    route_weight,
    expert_gate,
    expert_up,
    expert_down,
    dense_gate,
    dense_up,
    dense_down,
    gate_vector,
):
    tok_dev, width = tokens.shape
    top = routes.shape[1]
    half = width // lax.axis_size("tp")
    ep_count = lax.axis_size(EP)
    wide = lax.axis_size("ep_1")
    slots = ep_count * capacity
    units, hidden_units = dense_down.shape[0], expert_down.shape[1]
    core = lax.axis_index("tp").reshape(1)

    def exchange(rows):
        return lax.all_to_all(rows, EP, split_axis=0, concat_axis=0, tiled=True)

    def out(*dims, dtype=BF16):
        return pltpu.VMEM(dims, dtype)

    dma = pltpu.SemaphoreType.DMA
    outgoing, pack = call(
        functools.partial(first_kernel, wide),
        [out(ep_count, capacity, width), out(units, 3 * width + lane)],
        core,
        tokens,
        routes.T,
        norm_gain.reshape(-1, lane),
        gate_vector.reshape(1, -1),
        dense_gate.T,
        dense_up.T,
        dense_down,
        inside=7,
        scratch=(
            pltpu.VMEM((tok_dev, width), BF16),
            pltpu.VMEM((top, tok_dev), I32),
            pltpu.VMEM((width // lane, lane), F32),
            pltpu.VMEM((1, units), BF16),
            dma((7,)),
        ),
    )
    packs = [pack]
    for offset in shape[1:]:
        packs.append(from_chip(pack, *offset))
    mine = exchange(outgoing)
    gate, down = (
        pltpu.with_memory_space_constraint(w, pltpu.VMEM) for w in (expert_gate, expert_down)
    )
    other = swap_cores(mine)
    gate_pre, up_pre, up, combine = call(
        own_kernel,
        [out(slots, hidden_units, dtype=F32)] * 2
        + [out(width, hidden_units), out(tok_dev, slots, dtype=F32)],
        core,
        mine,
        gate,
        expert_up,
        routes.T,
        route_weight.T,
        inside=3,
        scratch=(
            pltpu.VMEM((top, tok_dev), I32),
            pltpu.VMEM((top, tok_dev), F32),
            dma((4,)),
        ),
    )
    act, expert_away = call(
        rest_kernel,
        [out(slots, hidden_units), out(slots, half)],
        core,
        other,
        gate_pre,
        up_pre,
        gate,
        up,
        down,
    )
    expert_away = swap_cores(expert_away)
    hidden, dense_away = call(
        dense_kernel,
        [out(slots, classes * units), out(slots, half + lane)],
        core,
        mine,
        other,
        *packs,
    )
    dense_away = swap_cores(dense_away)
    here = call(here_kernel, out(slots, width + lane), core, act, hidden, down, *packs)
    terms = call(join_kernel, out(ep_count, capacity, width + lane), here, expert_away, dense_away)
    returned = exchange(terms)
    return call(
        functools.partial(mix_kernel, wide),
        jax.ShapeDtypeStruct((tok_dev, half), BF16),
        returned,
        combine,
    )


def solution(mesh):
    side = math.isqrt(mesh.shape["ep"])
    split = Mesh(
        mesh.devices.reshape(mesh.shape["grp"], side, side, mesh.shape["tp"]),
        ("grp", "ep_0", "ep_1", "tp"),
    )
    placed = (
        P(GRP_EP, None),
        P(),
        P(GRP_EP, None),
        P(GRP_EP, None),
        P(EP, None, "tp"),
        P(EP, None, "tp"),
        P(EP, "tp", None),
        P(None, EP_TP),
        P(None, EP_TP),
        P(EP_TP, None),
        P(EP_TP),
    )

    return jax.shard_map(
        per_device, mesh=split, in_specs=placed, out_specs=P(GRP_EP, "tp"), check_vma=False
    )
```

```python
import functools
import math

import jax
import jax.numpy as jnp
from jax import lax
from jax.experimental import pallas as pl
from jax.experimental.pallas import tpu as pltpu
from jax.sharding import Mesh
from jax.sharding import PartitionSpec as P


EP = ("ep_0", "ep_1")
GRP_EP = ("grp", "ep_0", "ep_1")
EP_TP = ("ep_0", "ep_1", "tp")

clamp_limit = 7.0
sigmoid_slope = 1.702
norm_eps = 1e-06
capacity = 2
lane = 128
classes = 4

F32, BF16, I32 = jnp.float32, jnp.bfloat16, jnp.int32


def clamped_unit(gate_pre, up_pre):
    gated = jnp.minimum(gate_pre, clamp_limit)
    linear = jnp.clip(up_pre, -clamp_limit, clamp_limit)
    return (gated * jax.nn.sigmoid(sigmoid_slope * gated) * (linear + 1.0)).astype(BF16)


def dot(a, b):
    return lax.dot_general(a, b, (((1,), (0,)), ((), ())), preferred_element_type=F32)


def dot_nt(a, b):
    return lax.dot_general(a, b, (((1,), (1,)), ((), ())), preferred_element_type=F32)


def iota(dims, dim):
    return lax.broadcasted_iota(I32, dims, dim)


def swap_cores(value):
    return lax.ppermute(value, "tp", [(0, 1), (1, 0)])


def from_partner(value, partner):
    high, wide = lax.axis_size("ep_0"), lax.axis_size("ep_1")
    pairs = []
    for y in range(high):
        for x in range(wide):
            row, column = partner(y, x)
            pairs.append((y * wide + x, row % high * wide + column % wide))
    return lax.ppermute(value, EP, pairs)


partners = (
    lambda y, x: (y, x ^ 1),
    lambda y, x: (y, ((x + 1) ^ 1) - 1),
    lambda y, x: (y ^ 1, x),
)


def class_of(chip, wide):
    return (chip % wide + 2 * (chip // wide)) % classes


def copy_all(pairs, sems):
    copies = [pltpu.make_async_copy(src, dst, sems.at[n]) for n, (src, dst) in enumerate(pairs)]
    for copy in copies:
        copy.start()
    return copies


def first_kernel(
    wide,
    core,
    tokens_hbm,
    routes_hbm,
    gain_hbm,
    vector_hbm,
    gate_hbm,
    up_hbm,
    down_hbm,
    out,
    pack,
    tokens,
    routes,
    gain,
    vector,
    sems,
):
    tok_dev, width = tokens.shape
    copies = copy_all(
        (
            (routes_hbm, routes),
            (tokens_hbm, tokens),
            (gain_hbm, gain),
            (vector_hbm, vector),
            (gate_hbm, pack.at[:, :width]),
            (up_hbm, pack.at[:, width : 2 * width]),
            (down_hbm, pack.at[:, 2 * width : 3 * width]),
        ),
        sems,
    )
    half = width // 2
    top = routes.shape[0]
    ep_count = out.shape[0]
    slots = ep_count * capacity
    units = pack.shape[0]
    slot = iota((slots, tok_dev), 0)
    row = iota((slots, tok_dev), 1)
    expert = slot // capacity
    share = tok_dev // classes
    wanted = (row == class_of(expert, wide) * share + slot % capacity).astype(F32).astype(BF16)
    earlier = (iota((tok_dev, tok_dev), 0) < iota((tok_dev, tok_dev), 1)).astype(F32).astype(BF16)
    same = iota((units, units), 0) == iota((units, units), 1)
    lead = (iota((units, lane), 1) == 0).astype(F32).astype(BF16)
    copies[0].wait()
    member = jnp.zeros((slots, tok_dev), F32)
    for k in range(top):
        member = jnp.where(routes[k : k + 1, :] == expert, 1.0, member)
    rank = dot(member.astype(BF16), earlier)
    taken = jnp.where(rank == (slot % capacity).astype(F32), member, 0.0).astype(BF16)
    for copy in copies[1:4]:
        copy.wait()
    values = tokens[...].astype(F32)
    inverse = lax.rsqrt(jnp.mean(values * values, axis=-1, keepdims=True) + norm_eps)
    low = core[0] == 0
    mine = jnp.where(low, values[:, :half], values[:, half:]) * inverse
    blocks = half // lane
    normed = []
    for n in range(blocks):
        scale = jnp.where(low, gain[n : n + 1, :], gain[blocks + n : blocks + n + 1, :])
        normed.append((mine[:, n * lane : (n + 1) * lane] * scale).astype(BF16))
    normed = jnp.concatenate(normed, axis=1)
    spread = jnp.where(same, vector[...].astype(F32), 0.0).astype(BF16)
    pack[:, 3 * width :] = dot(spread, lead).astype(BF16)
    out[:, :, :half] = dot(taken, normed).astype(BF16).reshape(ep_count, capacity, half)
    out[:, :, half:] = dot(wanted, normed).astype(BF16).reshape(ep_count, capacity, half)
    for copy in copies[4:]:
        copy.wait()


def weigh(routes, weights, combine):
    top, tok_dev = routes.shape
    slots = combine.shape[1]
    slot = iota((tok_dev, slots), 1)
    eye = iota((tok_dev, tok_dev), 0) == iota((tok_dev, tok_dev), 1)
    earlier = (iota((tok_dev, tok_dev), 1) < iota((tok_dev, tok_dev), 0)).astype(F32).astype(BF16)
    member = jnp.zeros((tok_dev, slots), F32)
    weight = jnp.zeros((tok_dev, slots), F32)
    for k in range(top):
        named = jnp.sum(jnp.where(eye, routes[k : k + 1, :], 0), axis=1, keepdims=True)
        worth = jnp.sum(jnp.where(eye, weights[k : k + 1, :], 0.0), axis=1, keepdims=True)
        hit = named == slot // capacity
        member = jnp.where(hit, 1.0, member)
        weight = jnp.where(hit, worth, weight)
    rank = dot(earlier, member.astype(BF16))
    combine[...] = jnp.where(rank == (slot % capacity).astype(F32), weight, 0.0)


def halves(core, half):
    at = pl.multiple_of(core[0] * half, half)
    to = pl.multiple_of((1 - core[0]) * half, half)
    return at, to


def rows(packs, start, size):
    return jnp.concatenate([p[:, pl.ds(start, size)] for p in packs], axis=0)


def own_kernel(core, mine, gate, up_hbm, down_hbm, routes_hbm, weights_hbm, *refs):
    packs = refs[:classes]
    gate_pre, up_pre, dense_gate, dense_up, up, down, combine, routes, weights, sems = refs[classes:]
    half = mine.shape[2] // 2
    width = 2 * half
    at, to = halves(core, half)
    copies = copy_all(
        (
            (up_hbm.at[0, pl.ds(at, half), :], up.at[pl.ds(at, half), :]),
            (routes_hbm, routes),
            (weights_hbm, weights),
            (up_hbm.at[0, pl.ds(to, half), :], up.at[pl.ds(to, half), :]),
            (down_hbm.at[0, :, pl.ds(to, half)], down),
        ),
        sems,
    )
    x = mine[:, :, :half].reshape(-1, half)
    gate_pre[...] = dot(x, gate[0, pl.ds(at, half), :])
    z = mine[:, :, half:].reshape(-1, half)
    dense_gate[...] = dot_nt(z, rows(packs, at, half))
    dense_up[...] = dot_nt(z, rows(packs, width + at, half))
    copies[1].wait()
    copies[2].wait()
    weigh(routes, weights, combine)
    copies[0].wait()
    up_pre[...] = dot(x, up[pl.ds(at, half), :])
    for copy in copies[3:]:
        copy.wait()


def rest_kernel(core, other, gate_pre, up_pre, gate, up, down, act, away):
    half = other.shape[2] // 2
    _, to = halves(core, half)
    y = other[:, :, :half].reshape(-1, half)
    value = clamped_unit(
        gate_pre[...] + dot(y, gate[0, pl.ds(to, half), :]),
        up_pre[...] + dot(y, up[pl.ds(to, half), :]),
    )
    act[...] = value
    away[...] = dot(value, down[...]).astype(BF16)


def dense_kernel(core, other, dense_gate, dense_up, *refs):
    packs, (hidden, away) = refs[:classes], refs[classes:]
    half = other.shape[2] // 2
    width = 2 * half
    _, to = halves(core, half)
    z = other[:, :, half:].reshape(-1, half)
    value = clamped_unit(
        dense_gate[...] + dot_nt(z, rows(packs, to, half)),
        dense_up[...] + dot_nt(z, rows(packs, width + to, half)),
    )
    hidden[...] = value
    away[:, :half] = dot(value, rows(packs, 2 * width + to, half)).astype(BF16)
    away[:, half:] = dot(value, rows(packs, 3 * width, lane)).astype(BF16)


def here_kernel(core, act, hidden, down_hbm, *refs):
    packs, (out, down, sems) = refs[:classes], refs[classes:]
    half = down.shape[1]
    width = 2 * half
    at, _ = halves(core, half)
    (copy,) = copy_all(((down_hbm.at[0, :, pl.ds(at, half)], down),), sems)
    value = hidden[...]
    out[:, half:width] = dot(value, rows(packs, 2 * width + at, half)).astype(BF16)
    out[:, width:] = dot(value, rows(packs, 3 * width, lane)).astype(BF16)
    copy.wait()
    out[:, :half] = dot(act[...], down[...]).astype(BF16)


def join_kernel(here, expert_away, dense_away, out):
    half = expert_away.shape[1]
    shape3 = out.shape[:2] + (-1,)
    mine = here[...].astype(F32)
    expert = (mine[:, :half] + expert_away[...].astype(F32)).astype(BF16)
    dense = (mine[:, half:] + dense_away[...].astype(F32)).astype(BF16)
    out[:, :, :half] = expert.reshape(shape3)
    out[:, :, half:] = dense.reshape(shape3)


def mix_kernel(wide, returned, combine, out):
    tok_dev, half = out.shape
    slots = returned.shape[0] * returned.shape[1]
    slot = iota((tok_dev, slots), 1)
    share = tok_dev // classes
    owner = class_of(slot // capacity, wide) * share + slot % capacity
    wanted = (iota((tok_dev, slots), 0) == owner).astype(F32).astype(BF16)
    dense_out = dot(wanted, returned[:, :, half : 2 * half].reshape(slots, half))
    gate_logit = dot(wanted, returned[:, :, 2 * half :].reshape(slots, lane))[:, :1]
    first = combine[...].astype(BF16)
    rest = combine[...] - first.astype(F32)
    second = rest.astype(BF16)
    third = (rest - second.astype(F32)).astype(BF16)
    expert_rows = returned[:, :, :half].reshape(slots, half)
    expert_mix = dot(first, expert_rows) + (dot(second, expert_rows) + dot(third, expert_rows))
    out[...] = (jax.nn.sigmoid(gate_logit) * dense_out + expert_mix).astype(BF16)


def call(kernel, outs, *operands, inside=(), scratch=(), room=8 * 2**20):
    specs, placed = [], []
    for n, operand in enumerate(operands):
        if n in inside:
            specs.append(pl.BlockSpec(memory_space=pl.ANY))
            placed.append(pltpu.with_memory_space_constraint(operand, pltpu.HBM))
        elif operand.dtype == I32 and operand.ndim == 1:
            specs.append(pl.BlockSpec(memory_space=pltpu.SMEM))
            placed.append(operand)
        else:
            specs.append(pl.BlockSpec(memory_space=pltpu.VMEM))
            placed.append(operand)
    many = isinstance(outs, list)
    spec = pl.BlockSpec(memory_space=pltpu.VMEM)
    return pl.pallas_call(
        kernel,
        out_shape=outs,
        in_specs=specs,
        out_specs=[spec] * len(outs) if many else spec,
        scratch_shapes=list(scratch),
        cost_estimate=pl.CostEstimate(flops=10**9, transcendentals=0, bytes_accessed=0),
        compiler_params=pltpu.CompilerParams(vmem_limit_bytes=room),
    )(*placed)


def per_device(
    tokens,
    norm_gain,
    routes,
    route_weight,
    expert_gate,
    expert_up,
    expert_down,
    dense_gate,
    dense_up,
    dense_down,
    gate_vector,
):
    tok_dev, width = tokens.shape
    top = routes.shape[1]
    half = width // lax.axis_size("tp")
    ep_count = lax.axis_size(EP)
    wide = lax.axis_size("ep_1")
    slots = ep_count * capacity
    units, hidden_units = dense_down.shape[0], expert_down.shape[1]
    core = lax.axis_index("tp").reshape(1)

    def exchange(rows):
        return lax.all_to_all(rows, EP, split_axis=0, concat_axis=0, tiled=True)

    def out(*dims, dtype=BF16):
        return pltpu.VMEM(dims, dtype)

    dma = pltpu.SemaphoreType.DMA
    outgoing, pack = call(
        functools.partial(first_kernel, wide),
        [out(ep_count, capacity, width), out(units, 3 * width + lane)],
        core,
        tokens,
        routes.T,
        norm_gain.reshape(-1, lane),
        gate_vector.reshape(1, -1),
        dense_gate.T,
        dense_up.T,
        dense_down,
        inside=range(1, 8),
        scratch=(
            pltpu.VMEM((tok_dev, width), BF16),
            pltpu.VMEM((top, tok_dev), I32),
            pltpu.VMEM((width // lane, lane), F32),
            pltpu.VMEM((1, units), BF16),
            dma((7,)),
        ),
    )
    packs = [pack]
    for partner in partners:
        packs.append(from_partner(pack, partner))
    mine = exchange(outgoing)
    gate = pltpu.with_memory_space_constraint(expert_gate, pltpu.VMEM)
    other = swap_cores(mine)
    sums = [out(slots, hidden_units, dtype=F32)] * 2
    dense_sums = [out(slots, classes * units, dtype=F32)] * 2
    gate_pre, up_pre, dense_gate_pre, dense_up_pre, up, down, combine = call(
        own_kernel,
        sums
        + dense_sums
        + [
            out(width, hidden_units),
            out(hidden_units, half),
            out(tok_dev, slots, dtype=F32),
        ],
        core,
        mine,
        gate,
        expert_up,
        expert_down,
        routes.T,
        route_weight.T,
        *packs,
        inside=(3, 4, 5, 6),
        scratch=(
            pltpu.VMEM((top, tok_dev), I32),
            pltpu.VMEM((top, tok_dev), F32),
            dma((5,)),
        ),
    )
    hidden, dense_away = call(
        dense_kernel,
        [out(slots, classes * units), out(slots, half + lane)],
        core,
        other,
        dense_gate_pre,
        dense_up_pre,
        *packs,
    )
    dense_away = swap_cores(dense_away)
    act, expert_away = call(
        rest_kernel,
        [out(slots, hidden_units), out(slots, half)],
        core,
        other,
        gate_pre,
        up_pre,
        gate,
        up,
        down,
    )
    expert_away = swap_cores(expert_away)
    here = call(
        here_kernel,
        out(slots, width + lane),
        core,
        act,
        hidden,
        expert_down,
        *packs,
        inside=(3,),
        scratch=(pltpu.VMEM((hidden_units, half), BF16), dma((1,))),
    )
    terms = call(join_kernel, out(ep_count, capacity, width + lane), here, expert_away, dense_away)
    returned = exchange(terms)
    return call(
        functools.partial(mix_kernel, wide),
        jax.ShapeDtypeStruct((tok_dev, half), BF16),
        returned,
        combine,
    )


def solution(mesh):
    side = math.isqrt(mesh.shape["ep"])
    split = Mesh(
        mesh.devices.reshape(mesh.shape["grp"], side, side, mesh.shape["tp"]),
        ("grp", "ep_0", "ep_1", "tp"),
    )
    placed = (
        P(GRP_EP, None),
        P(),
        P(GRP_EP, None),
        P(GRP_EP, None),
        P(EP, None, "tp"),
        P(EP, None, "tp"),
        P(EP, "tp", None),
        P(None, EP_TP),
        P(None, EP_TP),
        P(EP_TP, None),
        P(EP_TP),
    )

    return jax.shard_map(
        per_device, mesh=split, in_specs=placed, out_specs=P(GRP_EP, "tp"), check_vma=False
    )
```

```python
import functools
import math

import jax
import jax.numpy as jnp
from jax import lax
from jax.experimental import pallas as pl
from jax.experimental.pallas import tpu as pltpu
from jax.sharding import Mesh
from jax.sharding import PartitionSpec as P


EP = ("ep_0", "ep_1")
GRP_EP = ("grp", "ep_0", "ep_1")
EP_TP = ("ep_0", "ep_1", "tp")

clamp_limit = 7.0
sigmoid_slope = 1.702
norm_eps = 1e-06
capacity = 2
lane = 128
classes = 4

F32, BF16, I32 = jnp.float32, jnp.bfloat16, jnp.int32


def clamped_unit(gate_pre, up_pre):
    gated = jnp.minimum(gate_pre, clamp_limit)
    linear = jnp.clip(up_pre, -clamp_limit, clamp_limit)
    return (gated * jax.nn.sigmoid(sigmoid_slope * gated) * (linear + 1.0)).astype(BF16)


def dot(a, b):
    return lax.dot_general(a, b, (((1,), (0,)), ((), ())), preferred_element_type=F32)


def dot_nt(a, b):
    return lax.dot_general(a, b, (((1,), (1,)), ((), ())), preferred_element_type=F32)


def iota(dims, dim):
    return lax.broadcasted_iota(I32, dims, dim)


def swap_cores(value):
    return lax.ppermute(value, "tp", [(0, 1), (1, 0)])


def from_partner(value, partner):
    high, wide = lax.axis_size("ep_0"), lax.axis_size("ep_1")
    pairs = []
    for y in range(high):
        for x in range(wide):
            row, column = partner(y, x)
            pairs.append((y * wide + x, row % high * wide + column % wide))
    return lax.ppermute(value, EP, pairs)


partners = (
    lambda y, x: (y, x ^ 1),
    lambda y, x: (y, ((x + 1) ^ 1) - 1),
    lambda y, x: (y ^ 1, x),
)


def expert_of(rank, high, wide):
    return rank % high * wide + rank // high


def class_of(chip, wide):
    return (chip % wide + 2 * (chip // wide)) % classes


def copy_all(pairs, sems):
    copies = [pltpu.make_async_copy(src, dst, sems.at[n]) for n, (src, dst) in enumerate(pairs)]
    for copy in copies:
        copy.start()
    return copies


def first_kernel(
    high,
    wide,
    core,
    tokens_hbm,
    routes_hbm,
    gain_hbm,
    vector_hbm,
    gate_hbm,
    up_hbm,
    down_hbm,
    out,
    pack,
    tokens,
    routes,
    gain,
    vector,
    sems,
):
    tok_dev, width = tokens.shape
    copies = copy_all(
        (
            (routes_hbm, routes),
            (tokens_hbm, tokens),
            (gain_hbm, gain),
            (vector_hbm, vector),
            (gate_hbm, pack.at[:, :width]),
            (up_hbm, pack.at[:, width : 2 * width]),
            (down_hbm, pack.at[:, 2 * width : 3 * width]),
        ),
        sems,
    )
    half = width // 2
    top = routes.shape[0]
    ep_count = out.shape[0]
    slots = ep_count * capacity
    units = pack.shape[0]
    slot = iota((slots, tok_dev), 0)
    row = iota((slots, tok_dev), 1)
    expert = expert_of(slot // capacity, high, wide)
    share = tok_dev // classes
    wanted = (row == class_of(expert, wide) * share + slot % capacity).astype(F32).astype(BF16)
    earlier = (iota((tok_dev, tok_dev), 0) < iota((tok_dev, tok_dev), 1)).astype(F32).astype(BF16)
    same = iota((units, units), 0) == iota((units, units), 1)
    lead = (iota((units, lane), 1) == 0).astype(F32).astype(BF16)
    copies[0].wait()
    member = jnp.zeros((slots, tok_dev), F32)
    for k in range(top):
        member = jnp.where(routes[k : k + 1, :] == expert, 1.0, member)
    rank = dot(member.astype(BF16), earlier)
    taken = jnp.where(rank == (slot % capacity).astype(F32), member, 0.0).astype(BF16)
    for copy in copies[1:4]:
        copy.wait()
    values = tokens[...].astype(F32)
    inverse = lax.rsqrt(jnp.mean(values * values, axis=-1, keepdims=True) + norm_eps)
    low = core[0] == 0
    mine = jnp.where(low, values[:, :half], values[:, half:]) * inverse
    blocks = half // lane
    normed = []
    for n in range(blocks):
        scale = jnp.where(low, gain[n : n + 1, :], gain[blocks + n : blocks + n + 1, :])
        normed.append((mine[:, n * lane : (n + 1) * lane] * scale).astype(BF16))
    normed = jnp.concatenate(normed, axis=1)
    spread = jnp.where(same, vector[...].astype(F32), 0.0).astype(BF16)
    pack[:, 3 * width :] = dot(spread, lead).astype(BF16)
    out[:, :, :half] = dot(taken, normed).astype(BF16).reshape(ep_count, capacity, half)
    out[:, :, half:] = dot(wanted, normed).astype(BF16).reshape(ep_count, capacity, half)
    for copy in copies[4:]:
        copy.wait()


def weigh(high, wide, routes, weights, combine):
    top, tok_dev = routes.shape
    slots = combine.shape[1]
    slot = iota((tok_dev, slots), 1)
    expert = expert_of(slot // capacity, high, wide)
    eye = iota((tok_dev, tok_dev), 0) == iota((tok_dev, tok_dev), 1)
    earlier = (iota((tok_dev, tok_dev), 1) < iota((tok_dev, tok_dev), 0)).astype(F32).astype(BF16)
    member = jnp.zeros((tok_dev, slots), F32)
    weight = jnp.zeros((tok_dev, slots), F32)
    for k in range(top):
        named = jnp.sum(jnp.where(eye, routes[k : k + 1, :], 0), axis=1, keepdims=True)
        worth = jnp.sum(jnp.where(eye, weights[k : k + 1, :], 0.0), axis=1, keepdims=True)
        hit = named == expert
        member = jnp.where(hit, 1.0, member)
        weight = jnp.where(hit, worth, weight)
    rank = dot(earlier, member.astype(BF16))
    combine[...] = jnp.where(rank == (slot % capacity).astype(F32), weight, 0.0)


def halves(core, half):
    at = pl.multiple_of(core[0] * half, half)
    to = pl.multiple_of((1 - core[0]) * half, half)
    return at, to


def rows(packs, start, size):
    return jnp.concatenate([p[:, pl.ds(start, size)] for p in packs], axis=0)


def own_kernel(high, wide, core, mine, gate, up, routes_hbm, weights_hbm, *refs):
    packs = refs[:classes]
    gate_pre, up_pre, dense_gate, dense_up, combine, routes, weights, sems = refs[classes:]
    half = mine.shape[2] // 2
    width = 2 * half
    at, _ = halves(core, half)
    copies = copy_all(((routes_hbm, routes), (weights_hbm, weights)), sems)
    x = mine[:, :, :half].reshape(-1, half)
    gate_pre[...] = dot(x, gate[0, pl.ds(at, half), :])
    up_pre[...] = dot(x, up[0, pl.ds(at, half), :])
    z = mine[:, :, half:].reshape(-1, half)
    dense_gate[...] = dot_nt(z, rows(packs, at, half))
    dense_up[...] = dot_nt(z, rows(packs, width + at, half))
    for copy in copies:
        copy.wait()
    weigh(high, wide, routes, weights, combine)


def rest_kernel(core, other, gate_pre, up_pre, gate, up, down, act, away):
    half = other.shape[2] // 2
    _, to = halves(core, half)
    y = other[:, :, :half].reshape(-1, half)
    value = clamped_unit(
        gate_pre[...] + dot(y, gate[0, pl.ds(to, half), :]),
        up_pre[...] + dot(y, up[0, pl.ds(to, half), :]),
    )
    act[...] = value
    away[...] = dot(value, down[0, :, pl.ds(to, half)]).astype(BF16)


def dense_kernel(core, other, dense_gate, dense_up, *refs):
    packs, (hidden, away) = refs[:classes], refs[classes:]
    half = other.shape[2] // 2
    width = 2 * half
    _, to = halves(core, half)
    z = other[:, :, half:].reshape(-1, half)
    value = clamped_unit(
        dense_gate[...] + dot_nt(z, rows(packs, to, half)),
        dense_up[...] + dot_nt(z, rows(packs, width + to, half)),
    )
    hidden[...] = value
    away[:, :half] = dot(value, rows(packs, 2 * width + to, half)).astype(BF16)
    away[:, half:] = dot(value, rows(packs, 3 * width, lane)).astype(BF16)


def here_kernel(core, act, hidden, down, *refs):
    packs, out = refs[:classes], refs[classes]
    half = down.shape[2] // 2
    width = 2 * half
    at, _ = halves(core, half)
    out[:, :half] = dot(act[...], down[0, :, pl.ds(at, half)]).astype(BF16)
    value = hidden[...]
    out[:, half:width] = dot(value, rows(packs, 2 * width + at, half)).astype(BF16)
    out[:, width:] = dot(value, rows(packs, 3 * width, lane)).astype(BF16)


def join_kernel(here, expert_away, dense_away, out):
    half = expert_away.shape[1]
    shape3 = out.shape[:2] + (-1,)
    mine = here[...].astype(F32)
    expert = (mine[:, :half] + expert_away[...].astype(F32)).astype(BF16)
    dense = (mine[:, half:] + dense_away[...].astype(F32)).astype(BF16)
    out[:, :, :half] = expert.reshape(shape3)
    out[:, :, half:] = dense.reshape(shape3)


def mix_kernel(high, wide, returned, combine, out):
    tok_dev, half = out.shape
    slots = returned.shape[0] * returned.shape[1]
    slot = iota((tok_dev, slots), 1)
    share = tok_dev // classes
    chip = expert_of(slot // capacity, high, wide)
    owner = class_of(chip, wide) * share + slot % capacity
    wanted = (iota((tok_dev, slots), 0) == owner).astype(F32).astype(BF16)
    dense_out = dot(wanted, returned[:, :, half : 2 * half].reshape(slots, half))
    gate_logit = dot(wanted, returned[:, :, 2 * half :].reshape(slots, lane))[:, :1]
    first = combine[...].astype(BF16)
    rest = combine[...] - first.astype(F32)
    second = rest.astype(BF16)
    third = (rest - second.astype(F32)).astype(BF16)
    expert_rows = returned[:, :, :half].reshape(slots, half)
    expert_mix = dot(first, expert_rows) + (dot(second, expert_rows) + dot(third, expert_rows))
    out[...] = (jax.nn.sigmoid(gate_logit) * dense_out + expert_mix).astype(BF16)


def call(kernel, outs, *operands, inside=(), scratch=(), room=8 * 2**20, flops=10**6):
    specs, placed = [], []
    for n, operand in enumerate(operands):
        if n in inside:
            specs.append(pl.BlockSpec(memory_space=pl.ANY))
            placed.append(pltpu.with_memory_space_constraint(operand, pltpu.HBM))
        elif operand.dtype == I32 and operand.ndim == 1:
            specs.append(pl.BlockSpec(memory_space=pltpu.SMEM))
            placed.append(operand)
        else:
            specs.append(pl.BlockSpec(memory_space=pltpu.VMEM))
            placed.append(operand)
    many = isinstance(outs, list)
    spec = pl.BlockSpec(memory_space=pltpu.VMEM)
    return pl.pallas_call(
        kernel,
        out_shape=outs,
        in_specs=specs,
        out_specs=[spec] * len(outs) if many else spec,
        scratch_shapes=list(scratch),
        cost_estimate=pl.CostEstimate(flops=flops, transcendentals=0, bytes_accessed=0),
        compiler_params=pltpu.CompilerParams(vmem_limit_bytes=room),
    )(*placed)


def per_device(
    tokens,
    norm_gain,
    routes,
    route_weight,
    expert_gate,
    expert_up,
    expert_down,
    dense_gate,
    dense_up,
    dense_down,
    gate_vector,
):
    tok_dev, width = tokens.shape
    top = routes.shape[1]
    half = width // lax.axis_size("tp")
    ep_count = lax.axis_size(EP)
    high, wide = lax.axis_size("ep_0"), lax.axis_size("ep_1")
    slots = ep_count * capacity
    units, hidden_units = dense_down.shape[0], expert_down.shape[1]
    core = lax.axis_index("tp").reshape(1)

    def exchange(rows):
        return lax.all_to_all(rows, EP[::-1], split_axis=0, concat_axis=0, tiled=True)

    def out(*dims, dtype=BF16):
        return pltpu.VMEM(dims, dtype)

    dma = pltpu.SemaphoreType.DMA
    outgoing, pack = call(
        functools.partial(first_kernel, high, wide),
        [out(ep_count, capacity, width), out(units, 3 * width + lane)],
        core,
        tokens,
        routes.T,
        norm_gain.reshape(-1, lane),
        gate_vector.reshape(1, -1),
        dense_gate.T,
        dense_up.T,
        dense_down,
        inside=range(1, 8),
        flops=10**11,
        scratch=(
            pltpu.VMEM((tok_dev, width), BF16),
            pltpu.VMEM((top, tok_dev), I32),
            pltpu.VMEM((width // lane, lane), F32),
            pltpu.VMEM((1, units), BF16),
            dma((7,)),
        ),
    )
    packs = [pack]
    for partner in partners:
        packs.append(from_partner(pack, partner))
    mine = exchange(outgoing)
    gate, up, down = (
        pltpu.with_memory_space_constraint(w, pltpu.VMEM)
        for w in (expert_gate, expert_up, expert_down)
    )
    other = swap_cores(mine)
    sums = [out(slots, hidden_units, dtype=F32)] * 2
    dense_sums = [out(slots, classes * units, dtype=F32)] * 2
    gate_pre, up_pre, dense_gate_pre, dense_up_pre, combine = call(
        functools.partial(own_kernel, high, wide),
        sums + dense_sums + [out(tok_dev, slots, dtype=F32)],
        core,
        mine,
        gate,
        up,
        routes.T,
        route_weight.T,
        *packs,
        inside=(4, 5),
        scratch=(
            pltpu.VMEM((top, tok_dev), I32),
            pltpu.VMEM((top, tok_dev), F32),
            dma((2,)),
        ),
    )
    hidden, dense_away = call(
        dense_kernel,
        [out(slots, classes * units), out(slots, half + lane)],
        core,
        other,
        dense_gate_pre,
        dense_up_pre,
        *packs,
    )
    dense_away = swap_cores(dense_away)
    act, expert_away = call(
        rest_kernel,
        [out(slots, hidden_units), out(slots, half)],
        core,
        other,
        gate_pre,
        up_pre,
        gate,
        up,
        down,
    )
    expert_away = swap_cores(expert_away)
    here = call(here_kernel, out(slots, width + lane), core, act, hidden, down, *packs)
    terms = call(join_kernel, out(ep_count, capacity, width + lane), here, expert_away, dense_away)
    returned = exchange(terms)
    return call(
        functools.partial(mix_kernel, high, wide),
        jax.ShapeDtypeStruct((tok_dev, half), BF16),
        returned,
        combine,
    )


def solution(mesh):
    side = math.isqrt(mesh.shape["ep"])
    split = Mesh(
        mesh.devices.reshape(mesh.shape["grp"], side, side, mesh.shape["tp"]),
        ("grp", "ep_0", "ep_1", "tp"),
    )
    placed = (
        P(GRP_EP, None),
        P(),
        P(GRP_EP, None),
        P(GRP_EP, None),
        P(EP, None, "tp"),
        P(EP, None, "tp"),
        P(EP, "tp", None),
        P(None, EP_TP),
        P(None, EP_TP),
        P(EP_TP, None),
        P(EP_TP),
    )

    return jax.shard_map(
        per_device, mesh=split, in_specs=placed, out_specs=P(GRP_EP, "tp"), check_vma=False
    )
```

```python
import functools
import math

import jax
import jax.numpy as jnp
from jax import lax
from jax.experimental import pallas as pl
from jax.experimental.pallas import tpu as pltpu
from jax.sharding import Mesh
from jax.sharding import PartitionSpec as P


EP = ("ep_0", "ep_1")
GRP_EP = ("grp", "ep_0", "ep_1")
EP_TP = ("ep_0", "ep_1", "tp")

clamp_limit = 7.0
sigmoid_slope = 1.702
norm_eps = 1e-06
capacity = 2
lane = 128
classes = 4

F32, BF16, I32 = jnp.float32, jnp.bfloat16, jnp.int32


def clamped_unit(gate_pre, up_pre):
    gated = jnp.minimum(gate_pre, clamp_limit)
    linear = jnp.clip(up_pre, -clamp_limit, clamp_limit)
    return (gated * jax.nn.sigmoid(sigmoid_slope * gated) * (linear + 1.0)).astype(BF16)


def dot(a, b):
    return lax.dot_general(a, b, (((1,), (0,)), ((), ())), preferred_element_type=F32)


def dot_nt(a, b):
    return lax.dot_general(a, b, (((1,), (1,)), ((), ())), preferred_element_type=F32)


def iota(dims, dim):
    return lax.broadcasted_iota(I32, dims, dim)


def swap_cores(value):
    return lax.ppermute(value, "tp", [(0, 1), (1, 0)])


def from_partner(value, partner):
    high, wide = lax.axis_size("ep_0"), lax.axis_size("ep_1")
    pairs = []
    for y in range(high):
        for x in range(wide):
            row, column = partner(y, x)
            pairs.append((y * wide + x, row % high * wide + column % wide))
    return lax.ppermute(value, EP, pairs)


partners = (
    lambda y, x: (y, x + 1),
    lambda y, x: (y + 1, x),
    lambda y, x: (y, x - 1),
)


def expert_of(rank, high, wide):
    return rank % high * wide + rank // high


def class_of(chip, wide):
    return (chip % wide + 2 * (chip // wide)) % classes


def copy_all(pairs, sems):
    copies = [pltpu.make_async_copy(src, dst, sems.at[n]) for n, (src, dst) in enumerate(pairs)]
    for copy in copies:
        copy.start()
    return copies


def first_kernel(
    high,
    wide,
    core,
    tokens_hbm,
    routes_hbm,
    gain_hbm,
    vector_hbm,
    gate_hbm,
    up_hbm,
    down_hbm,
    out,
    pack,
    tokens,
    routes,
    gain,
    vector,
    sems,
):
    tok_dev, width = tokens.shape
    copies = copy_all(
        (
            (routes_hbm, routes),
            (tokens_hbm, tokens),
            (gain_hbm, gain),
            (vector_hbm, vector),
            (gate_hbm, pack.at[:, :width]),
            (up_hbm, pack.at[:, width : 2 * width]),
            (down_hbm, pack.at[:, 2 * width : 3 * width]),
        ),
        sems,
    )
    half = width // 2
    top = routes.shape[0]
    ep_count = out.shape[0]
    slots = ep_count * capacity
    units = pack.shape[0]
    slot = iota((slots, tok_dev), 0)
    row = iota((slots, tok_dev), 1)
    expert = expert_of(slot // capacity, high, wide)
    share = tok_dev // classes
    wanted = (row == class_of(expert, wide) * share + slot % capacity).astype(F32).astype(BF16)
    earlier = (iota((tok_dev, tok_dev), 0) < iota((tok_dev, tok_dev), 1)).astype(F32).astype(BF16)
    same = iota((units, units), 0) == iota((units, units), 1)
    lead = (iota((units, lane), 1) == 0).astype(F32).astype(BF16)
    copies[0].wait()
    member = jnp.zeros((slots, tok_dev), F32)
    for k in range(top):
        member = jnp.where(routes[k : k + 1, :] == expert, 1.0, member)
    rank = dot(member.astype(BF16), earlier)
    taken = jnp.where(rank == (slot % capacity).astype(F32), member, 0.0).astype(BF16)
    for copy in copies[1:4]:
        copy.wait()
    values = tokens[...].astype(F32)
    inverse = lax.rsqrt(jnp.mean(values * values, axis=-1, keepdims=True) + norm_eps)
    low = core[0] == 0
    mine = jnp.where(low, values[:, :half], values[:, half:]) * inverse
    blocks = half // lane
    normed = []
    for n in range(blocks):
        scale = jnp.where(low, gain[n : n + 1, :], gain[blocks + n : blocks + n + 1, :])
        normed.append((mine[:, n * lane : (n + 1) * lane] * scale).astype(BF16))
    normed = jnp.concatenate(normed, axis=1)
    spread = jnp.where(same, vector[...].astype(F32), 0.0).astype(BF16)
    pack[:, 3 * width :] = dot(spread, lead).astype(BF16)
    out[:, :, :half] = dot(taken, normed).astype(BF16).reshape(ep_count, capacity, half)
    out[:, :, half:] = dot(wanted, normed).astype(BF16).reshape(ep_count, capacity, half)
    for copy in copies[4:]:
        copy.wait()


def weigh(high, wide, routes, weights, combine):
    top, tok_dev = routes.shape
    slots = combine.shape[1]
    slot = iota((tok_dev, slots), 1)
    expert = expert_of(slot // capacity, high, wide)
    eye = iota((tok_dev, tok_dev), 0) == iota((tok_dev, tok_dev), 1)
    earlier = (iota((tok_dev, tok_dev), 1) < iota((tok_dev, tok_dev), 0)).astype(F32).astype(BF16)
    member = jnp.zeros((tok_dev, slots), F32)
    weight = jnp.zeros((tok_dev, slots), F32)
    for k in range(top):
        named = jnp.sum(jnp.where(eye, routes[k : k + 1, :], 0), axis=1, keepdims=True)
        worth = jnp.sum(jnp.where(eye, weights[k : k + 1, :], 0.0), axis=1, keepdims=True)
        hit = named == expert
        member = jnp.where(hit, 1.0, member)
        weight = jnp.where(hit, worth, weight)
    rank = dot(earlier, member.astype(BF16))
    combine[...] = jnp.where(rank == (slot % capacity).astype(F32), weight, 0.0)


def halves(core, half):
    at = pl.multiple_of(core[0] * half, half)
    to = pl.multiple_of((1 - core[0]) * half, half)
    return at, to


def rows(packs, start, size):
    return jnp.concatenate([p[:, pl.ds(start, size)] for p in packs], axis=0)


def own_kernel(high, wide, core, mine, gate, up, routes_hbm, weights_hbm, *refs):
    packs = refs[:classes]
    gate_pre, up_pre, dense_gate, dense_up, combine, routes, weights, sems = refs[classes:]
    half = mine.shape[2] // 2
    width = 2 * half
    at, _ = halves(core, half)
    copies = copy_all(((routes_hbm, routes), (weights_hbm, weights)), sems)
    x = mine[:, :, :half].reshape(-1, half)
    gate_pre[...] = dot(x, gate[0, pl.ds(at, half), :])
    up_pre[...] = dot(x, up[0, pl.ds(at, half), :])
    z = mine[:, :, half:].reshape(-1, half)
    dense_gate[...] = dot_nt(z, rows(packs, at, half))
    dense_up[...] = dot_nt(z, rows(packs, width + at, half))
    for copy in copies:
        copy.wait()
    weigh(high, wide, routes, weights, combine)


def rest_kernel(core, other, gate_pre, up_pre, gate, up, down, act, away):
    half = other.shape[2] // 2
    _, to = halves(core, half)
    y = other[:, :, :half].reshape(-1, half)
    value = clamped_unit(
        gate_pre[...] + dot(y, gate[0, pl.ds(to, half), :]),
        up_pre[...] + dot(y, up[0, pl.ds(to, half), :]),
    )
    act[...] = value
    away[...] = dot(value, down[0, :, pl.ds(to, half)]).astype(BF16)


def dense_kernel(core, other, dense_gate, dense_up, *refs):
    packs, (hidden, away) = refs[:classes], refs[classes:]
    half = other.shape[2] // 2
    width = 2 * half
    _, to = halves(core, half)
    z = other[:, :, half:].reshape(-1, half)
    value = clamped_unit(
        dense_gate[...] + dot_nt(z, rows(packs, to, half)),
        dense_up[...] + dot_nt(z, rows(packs, width + to, half)),
    )
    hidden[...] = value
    away[:, :half] = dot(value, rows(packs, 2 * width + to, half)).astype(BF16)
    away[:, half:] = dot(value, rows(packs, 3 * width, lane)).astype(BF16)


def here_kernel(core, act, hidden, down, *refs):
    packs, out = refs[:classes], refs[classes]
    half = down.shape[2] // 2
    width = 2 * half
    at, _ = halves(core, half)
    out[:, :half] = dot(act[...], down[0, :, pl.ds(at, half)]).astype(BF16)
    value = hidden[...]
    out[:, half:width] = dot(value, rows(packs, 2 * width + at, half)).astype(BF16)
    out[:, width:] = dot(value, rows(packs, 3 * width, lane)).astype(BF16)


def join_kernel(here, expert_away, dense_away, out):
    half = expert_away.shape[1]
    shape3 = out.shape[:2] + (-1,)
    mine = here[...].astype(F32)
    expert = (mine[:, :half] + expert_away[...].astype(F32)).astype(BF16)
    dense = (mine[:, half:] + dense_away[...].astype(F32)).astype(BF16)
    out[:, :, :half] = expert.reshape(shape3)
    out[:, :, half:] = dense.reshape(shape3)


def mix_kernel(high, wide, returned, combine, out):
    tok_dev, half = out.shape
    slots = returned.shape[0] * returned.shape[1]
    slot = iota((tok_dev, slots), 1)
    share = tok_dev // classes
    chip = expert_of(slot // capacity, high, wide)
    owner = class_of(chip, wide) * share + slot % capacity
    wanted = (iota((tok_dev, slots), 0) == owner).astype(F32).astype(BF16)
    dense_out = dot(wanted, returned[:, :, half : 2 * half].reshape(slots, half))
    gate_logit = dot(wanted, returned[:, :, 2 * half :].reshape(slots, lane))[:, :1]
    first = combine[...].astype(BF16)
    rest = combine[...] - first.astype(F32)
    second = rest.astype(BF16)
    third = (rest - second.astype(F32)).astype(BF16)
    terms = [first.astype(F32), second.astype(F32), third.astype(F32)]
    stacked = jnp.concatenate(terms, axis=0).astype(BF16)
    parts = dot(stacked, returned[:, :, :half].reshape(slots, half))
    expert_mix = parts[:tok_dev] + (parts[tok_dev : 2 * tok_dev] + parts[2 * tok_dev :])
    out[...] = (jax.nn.sigmoid(gate_logit) * dense_out + expert_mix).astype(BF16)


def call(kernel, outs, *operands, inside=(), scratch=(), room=8 * 2**20, flops=10**6):
    specs, placed = [], []
    for n, operand in enumerate(operands):
        if n in inside:
            specs.append(pl.BlockSpec(memory_space=pl.ANY))
            placed.append(pltpu.with_memory_space_constraint(operand, pltpu.HBM))
        elif operand.dtype == I32 and operand.ndim == 1:
            specs.append(pl.BlockSpec(memory_space=pltpu.SMEM))
            placed.append(operand)
        else:
            specs.append(pl.BlockSpec(memory_space=pltpu.VMEM))
            placed.append(operand)
    many = isinstance(outs, list)
    spec = pl.BlockSpec(memory_space=pltpu.VMEM)
    return pl.pallas_call(
        kernel,
        out_shape=outs,
        in_specs=specs,
        out_specs=[spec] * len(outs) if many else spec,
        scratch_shapes=list(scratch),
        cost_estimate=pl.CostEstimate(flops=flops, transcendentals=0, bytes_accessed=0),
        compiler_params=pltpu.CompilerParams(vmem_limit_bytes=room),
    )(*placed)


def per_device(
    tokens,
    norm_gain,
    routes,
    route_weight,
    expert_gate,
    expert_up,
    expert_down,
    dense_gate,
    dense_up,
    dense_down,
    gate_vector,
):
    tok_dev, width = tokens.shape
    top = routes.shape[1]
    half = width // lax.axis_size("tp")
    ep_count = lax.axis_size(EP)
    high, wide = lax.axis_size("ep_0"), lax.axis_size("ep_1")
    slots = ep_count * capacity
    units, hidden_units = dense_down.shape[0], expert_down.shape[1]
    core = lax.axis_index("tp").reshape(1)

    def exchange(rows):
        return lax.all_to_all(rows, EP[::-1], split_axis=0, concat_axis=0, tiled=True)

    def out(*dims, dtype=BF16):
        return pltpu.VMEM(dims, dtype)

    dma = pltpu.SemaphoreType.DMA
    outgoing, pack = call(
        functools.partial(first_kernel, high, wide),
        [out(ep_count, capacity, width), out(units, 3 * width + lane)],
        core,
        tokens,
        routes.T,
        norm_gain.reshape(-1, lane),
        gate_vector.reshape(1, -1),
        dense_gate.T,
        dense_up.T,
        dense_down,
        inside=range(1, 8),
        flops=10**11,
        scratch=(
            pltpu.VMEM((tok_dev, width), BF16),
            pltpu.VMEM((top, tok_dev), I32),
            pltpu.VMEM((width // lane, lane), F32),
            pltpu.VMEM((1, units), BF16),
            dma((7,)),
        ),
    )
    packs = [pack]
    for partner in partners:
        packs.append(from_partner(pack, partner))
    mine = exchange(outgoing)
    gate, up, down = (
        pltpu.with_memory_space_constraint(w, pltpu.VMEM)
        for w in (expert_gate, expert_up, expert_down)
    )
    other = swap_cores(mine)
    sums = [out(slots, hidden_units, dtype=F32)] * 2
    dense_sums = [out(slots, classes * units, dtype=F32)] * 2
    gate_pre, up_pre, dense_gate_pre, dense_up_pre, combine = call(
        functools.partial(own_kernel, high, wide),
        sums + dense_sums + [out(tok_dev, slots, dtype=F32)],
        core,
        mine,
        gate,
        up,
        routes.T,
        route_weight.T,
        *packs,
        inside=(4, 5),
        scratch=(
            pltpu.VMEM((top, tok_dev), I32),
            pltpu.VMEM((top, tok_dev), F32),
            dma((2,)),
        ),
    )
    hidden, dense_away = call(
        dense_kernel,
        [out(slots, classes * units), out(slots, half + lane)],
        core,
        other,
        dense_gate_pre,
        dense_up_pre,
        *packs,
    )
    dense_away = swap_cores(dense_away)
    act, expert_away = call(
        rest_kernel,
        [out(slots, hidden_units), out(slots, half)],
        core,
        other,
        gate_pre,
        up_pre,
        gate,
        up,
        down,
    )
    expert_away = swap_cores(expert_away)
    here = call(here_kernel, out(slots, width + lane), core, act, hidden, down, *packs)
    terms = call(join_kernel, out(ep_count, capacity, width + lane), here, expert_away, dense_away)
    returned = exchange(terms)
    return call(
        functools.partial(mix_kernel, high, wide),
        jax.ShapeDtypeStruct((tok_dev, half), BF16),
        returned,
        combine,
    )


def solution(mesh):
    side = math.isqrt(mesh.shape["ep"])
    split = Mesh(
        mesh.devices.reshape(mesh.shape["grp"], side, side, mesh.shape["tp"]),
        ("grp", "ep_0", "ep_1", "tp"),
    )
    placed = (
        P(GRP_EP, None),
        P(),
        P(GRP_EP, None),
        P(GRP_EP, None),
        P(EP, None, "tp"),
        P(EP, None, "tp"),
        P(EP, "tp", None),
        P(None, EP_TP),
        P(None, EP_TP),
        P(EP_TP, None),
        P(EP_TP),
    )

    return jax.shard_map(
        per_device, mesh=split, in_specs=placed, out_specs=P(GRP_EP, "tp"), check_vma=False
    )
```

```python
import functools
import math

import jax
import jax.numpy as jnp
from jax import lax
from jax.experimental import pallas as pl
from jax.experimental.pallas import tpu as pltpu
from jax.sharding import Mesh
from jax.sharding import PartitionSpec as P


EP = ("ep_0", "ep_1")
GRP_EP = ("grp", "ep_0", "ep_1")
EP_TP = ("ep_0", "ep_1", "tp")

clamp_limit = 7.0
sigmoid_slope = 1.702
norm_eps = 1e-06
capacity = 2
lane = 128
classes = 4

F32, BF16, I32 = jnp.float32, jnp.bfloat16, jnp.int32


def clamped_unit(gate_pre, up_pre):
    gated = jnp.minimum(gate_pre, clamp_limit)
    linear = jnp.clip(up_pre, -clamp_limit, clamp_limit)
    return (gated * jax.nn.sigmoid(sigmoid_slope * gated) * (linear + 1.0)).astype(BF16)


def dot(a, b):
    return lax.dot_general(a, b, (((1,), (0,)), ((), ())), preferred_element_type=F32)


def dot_nt(a, b):
    return lax.dot_general(a, b, (((1,), (1,)), ((), ())), preferred_element_type=F32)


def iota(dims, dim):
    return lax.broadcasted_iota(I32, dims, dim)


def swap_cores(value):
    return lax.ppermute(value, "tp", [(0, 1), (1, 0)])


def from_partner(value, partner):
    high, wide = lax.axis_size("ep_0"), lax.axis_size("ep_1")
    pairs = []
    for y in range(high):
        for x in range(wide):
            row, column = partner(y, x)
            pairs.append((y * wide + x, row % high * wide + column % wide))
    return lax.ppermute(value, EP, pairs)


partners = (
    lambda y, x: (y, x ^ 1),
    lambda y, x: (y, ((x + 1) ^ 1) - 1),
    lambda y, x: (y ^ 1, x),
)


def expert_of(rank, high, wide):
    return rank % high * wide + rank // high


def class_of(chip, wide):
    return (chip % wide + 2 * (chip // wide)) % classes


def copy_all(pairs, sems):
    copies = [pltpu.make_async_copy(src, dst, sems.at[n]) for n, (src, dst) in enumerate(pairs)]
    for copy in copies:
        copy.start()
    return copies


def first_kernel(
    high,
    wide,
    core,
    tokens_hbm,
    routes_hbm,
    gain_hbm,
    vector_hbm,
    gate_hbm,
    up_hbm,
    down_hbm,
    out,
    pack,
    tokens,
    routes,
    gain,
    vector,
    sems,
):
    tok_dev, width = tokens.shape
    copies = copy_all(
        (
            (routes_hbm, routes),
            (tokens_hbm, tokens),
            (gain_hbm, gain),
            (vector_hbm, vector),
            (gate_hbm, pack.at[:, :width]),
            (up_hbm, pack.at[:, width : 2 * width]),
            (down_hbm, pack.at[:, 2 * width : 3 * width]),
        ),
        sems,
    )
    half = width // 2
    top = routes.shape[0]
    ep_count = out.shape[0]
    slots = ep_count * capacity
    units = pack.shape[0]
    slot = iota((slots, tok_dev), 0)
    row = iota((slots, tok_dev), 1)
    expert = expert_of(slot // capacity, high, wide)
    share = tok_dev // classes
    wanted = (row == class_of(expert, wide) * share + slot % capacity).astype(F32).astype(BF16)
    earlier = (iota((tok_dev, tok_dev), 0) < iota((tok_dev, tok_dev), 1)).astype(F32).astype(BF16)
    same = iota((units, units), 0) == iota((units, units), 1)
    lead = (iota((units, lane), 1) == 0).astype(F32).astype(BF16)
    copies[0].wait()
    member = jnp.zeros((slots, tok_dev), F32)
    for k in range(top):
        member = jnp.where(routes[k : k + 1, :] == expert, 1.0, member)
    rank = dot(member.astype(BF16), earlier)
    taken = jnp.where(rank == (slot % capacity).astype(F32), member, 0.0).astype(BF16)
    for copy in copies[1:4]:
        copy.wait()
    values = tokens[...].astype(F32)
    inverse = lax.rsqrt(jnp.mean(values * values, axis=-1, keepdims=True) + norm_eps)
    low = core[0] == 0
    mine = jnp.where(low, values[:, :half], values[:, half:]) * inverse
    blocks = half // lane
    normed = []
    for n in range(blocks):
        scale = jnp.where(low, gain[n : n + 1, :], gain[blocks + n : blocks + n + 1, :])
        normed.append((mine[:, n * lane : (n + 1) * lane] * scale).astype(BF16))
    normed = jnp.concatenate(normed, axis=1)
    spread = jnp.where(same, vector[...].astype(F32), 0.0).astype(BF16)
    pack[:, 3 * width :] = dot(spread, lead).astype(BF16)
    picked = dot(jnp.concatenate([taken, wanted], axis=0), normed).astype(BF16)
    out[:, :, :half] = picked[:slots].reshape(ep_count, capacity, half)
    out[:, :, half:] = picked[slots:].reshape(ep_count, capacity, half)
    for copy in copies[4:]:
        copy.wait()


def weigh(high, wide, routes, weights, combine):
    top, tok_dev = routes.shape
    slots = combine.shape[1]
    slot = iota((tok_dev, slots), 1)
    expert = expert_of(slot // capacity, high, wide)
    eye = iota((tok_dev, tok_dev), 0) == iota((tok_dev, tok_dev), 1)
    earlier = (iota((tok_dev, tok_dev), 1) < iota((tok_dev, tok_dev), 0)).astype(F32).astype(BF16)
    member = jnp.zeros((tok_dev, slots), F32)
    weight = jnp.zeros((tok_dev, slots), F32)
    for k in range(top):
        named = jnp.sum(jnp.where(eye, routes[k : k + 1, :], 0), axis=1, keepdims=True)
        worth = jnp.sum(jnp.where(eye, weights[k : k + 1, :], 0.0), axis=1, keepdims=True)
        hit = named == expert
        member = jnp.where(hit, 1.0, member)
        weight = jnp.where(hit, worth, weight)
    rank = dot(earlier, member.astype(BF16))
    combine[...] = jnp.where(rank == (slot % capacity).astype(F32), weight, 0.0)


def halves(core, half):
    at = pl.multiple_of(core[0] * half, half)
    to = pl.multiple_of((1 - core[0]) * half, half)
    return at, to


def rows(packs, start, size):
    return jnp.concatenate([p[:, pl.ds(start, size)] for p in packs], axis=0)


def own_kernel(high, wide, core, mine, gate, up, routes_hbm, weights_hbm, *refs):
    packs = refs[:classes]
    gate_pre, up_pre, dense_gate, dense_up, combine, routes, weights, sems = refs[classes:]
    half = mine.shape[2] // 2
    width = 2 * half
    at, _ = halves(core, half)
    copies = copy_all(((routes_hbm, routes), (weights_hbm, weights)), sems)
    x = mine[:, :, :half].reshape(-1, half)
    gate_pre[...] = dot(x, gate[0, pl.ds(at, half), :])
    up_pre[...] = dot(x, up[0, pl.ds(at, half), :])
    z = mine[:, :, half:].reshape(-1, half)
    dense_gate[...] = dot_nt(z, rows(packs, at, half))
    dense_up[...] = dot_nt(z, rows(packs, width + at, half))
    for copy in copies:
        copy.wait()
    weigh(high, wide, routes, weights, combine)


def rest_kernel(core, other, gate_pre, up_pre, gate, up, down, act, away):
    half = other.shape[2] // 2
    _, to = halves(core, half)
    y = other[:, :, :half].reshape(-1, half)
    value = clamped_unit(
        gate_pre[...] + dot(y, gate[0, pl.ds(to, half), :]),
        up_pre[...] + dot(y, up[0, pl.ds(to, half), :]),
    )
    act[...] = value
    away[...] = dot(value, down[0, :, pl.ds(to, half)]).astype(BF16)


def dense_kernel(core, other, dense_gate, dense_up, *refs):
    packs, (hidden, away) = refs[:classes], refs[classes:]
    half = other.shape[2] // 2
    width = 2 * half
    _, to = halves(core, half)
    z = other[:, :, half:].reshape(-1, half)
    value = clamped_unit(
        dense_gate[...] + dot_nt(z, rows(packs, to, half)),
        dense_up[...] + dot_nt(z, rows(packs, width + to, half)),
    )
    hidden[...] = value
    away[:, :half] = dot(value, rows(packs, 2 * width + to, half)).astype(BF16)
    away[:, half:] = dot(value, rows(packs, 3 * width, lane)).astype(BF16)


def here_kernel(core, act, hidden, down, *refs):
    packs, out = refs[:classes], refs[classes]
    half = down.shape[2] // 2
    width = 2 * half
    at, _ = halves(core, half)
    out[:, :half] = dot(act[...], down[0, :, pl.ds(at, half)]).astype(BF16)
    value = hidden[...]
    out[:, half:width] = dot(value, rows(packs, 2 * width + at, half)).astype(BF16)
    out[:, width:] = dot(value, rows(packs, 3 * width, lane)).astype(BF16)


def join_kernel(here, expert_away, dense_away, out):
    half = expert_away.shape[1]
    shape3 = out.shape[:2] + (-1,)
    mine = here[...].astype(F32)
    expert = (mine[:, :half] + expert_away[...].astype(F32)).astype(BF16)
    dense = (mine[:, half:] + dense_away[...].astype(F32)).astype(BF16)
    out[:, :, :half] = expert.reshape(shape3)
    out[:, :, half:] = dense.reshape(shape3)


def mix_kernel(high, wide, returned, combine, out):
    tok_dev, half = out.shape
    slots = returned.shape[0] * returned.shape[1]
    slot = iota((tok_dev, slots), 1)
    share = tok_dev // classes
    chip = expert_of(slot // capacity, high, wide)
    owner = class_of(chip, wide) * share + slot % capacity
    wanted = (iota((tok_dev, slots), 0) == owner).astype(F32).astype(BF16)
    dense_out = dot(wanted, returned[:, :, half : 2 * half].reshape(slots, half))
    gate_logit = dot(wanted, returned[:, :, 2 * half :].reshape(slots, lane))[:, :1]
    first = combine[...].astype(BF16)
    rest = combine[...] - first.astype(F32)
    second = rest.astype(BF16)
    third = (rest - second.astype(F32)).astype(BF16)
    expert_rows = returned[:, :, :half].reshape(slots, half)
    expert_mix = dot(first, expert_rows) + (dot(second, expert_rows) + dot(third, expert_rows))
    out[...] = (jax.nn.sigmoid(gate_logit) * dense_out + expert_mix).astype(BF16)


def call(kernel, outs, *operands, inside=(), scratch=(), room=8 * 2**20, flops=10**6):
    specs, placed = [], []
    for n, operand in enumerate(operands):
        if n in inside:
            specs.append(pl.BlockSpec(memory_space=pl.ANY))
            placed.append(pltpu.with_memory_space_constraint(operand, pltpu.HBM))
        elif operand.dtype == I32 and operand.ndim == 1:
            specs.append(pl.BlockSpec(memory_space=pltpu.SMEM))
            placed.append(operand)
        else:
            specs.append(pl.BlockSpec(memory_space=pltpu.VMEM))
            placed.append(operand)
    many = isinstance(outs, list)
    spec = pl.BlockSpec(memory_space=pltpu.VMEM)
    return pl.pallas_call(
        kernel,
        out_shape=outs,
        in_specs=specs,
        out_specs=[spec] * len(outs) if many else spec,
        scratch_shapes=list(scratch),
        cost_estimate=pl.CostEstimate(flops=flops, transcendentals=0, bytes_accessed=0),
        compiler_params=pltpu.CompilerParams(vmem_limit_bytes=room),
    )(*placed)


def per_device(
    tokens,
    norm_gain,
    routes,
    route_weight,
    expert_gate,
    expert_up,
    expert_down,
    dense_gate,
    dense_up,
    dense_down,
    gate_vector,
):
    tok_dev, width = tokens.shape
    top = routes.shape[1]
    half = width // lax.axis_size("tp")
    ep_count = lax.axis_size(EP)
    high, wide = lax.axis_size("ep_0"), lax.axis_size("ep_1")
    slots = ep_count * capacity
    units, hidden_units = dense_down.shape[0], expert_down.shape[1]
    core = lax.axis_index("tp").reshape(1)

    def exchange(rows):
        return lax.all_to_all(rows, EP[::-1], split_axis=0, concat_axis=0, tiled=True)

    def out(*dims, dtype=BF16):
        return pltpu.VMEM(dims, dtype)

    dma = pltpu.SemaphoreType.DMA
    outgoing, pack = call(
        functools.partial(first_kernel, high, wide),
        [out(ep_count, capacity, width), out(units, 3 * width + lane)],
        core,
        tokens,
        routes.T,
        norm_gain.reshape(-1, lane),
        gate_vector.reshape(1, -1),
        dense_gate.T,
        dense_up.T,
        dense_down,
        inside=range(1, 8),
        flops=10**11,
        scratch=(
            pltpu.VMEM((tok_dev, width), BF16),
            pltpu.VMEM((top, tok_dev), I32),
            pltpu.VMEM((width // lane, lane), F32),
            pltpu.VMEM((1, units), BF16),
            dma((7,)),
        ),
    )
    packs = [pack]
    for partner in partners:
        packs.append(from_partner(pack, partner))
    mine = exchange(outgoing)
    gate, up, down = (
        pltpu.with_memory_space_constraint(w, pltpu.VMEM)
        for w in (expert_gate, expert_up, expert_down)
    )
    other = swap_cores(mine)
    sums = [out(slots, hidden_units, dtype=F32)] * 2
    dense_sums = [out(slots, classes * units, dtype=F32)] * 2
    gate_pre, up_pre, dense_gate_pre, dense_up_pre, combine = call(
        functools.partial(own_kernel, high, wide),
        sums + dense_sums + [out(tok_dev, slots, dtype=F32)],
        core,
        mine,
        gate,
        up,
        routes.T,
        route_weight.T,
        *packs,
        inside=(4, 5),
        scratch=(
            pltpu.VMEM((top, tok_dev), I32),
            pltpu.VMEM((top, tok_dev), F32),
            dma((2,)),
        ),
    )
    hidden, dense_away = call(
        dense_kernel,
        [out(slots, classes * units), out(slots, half + lane)],
        core,
        other,
        dense_gate_pre,
        dense_up_pre,
        *packs,
    )
    dense_away = swap_cores(dense_away)
    act, expert_away = call(
        rest_kernel,
        [out(slots, hidden_units), out(slots, half)],
        core,
        other,
        gate_pre,
        up_pre,
        gate,
        up,
        down,
    )
    expert_away = swap_cores(expert_away)
    here = call(here_kernel, out(slots, width + lane), core, act, hidden, down, *packs)
    terms = call(join_kernel, out(ep_count, capacity, width + lane), here, expert_away, dense_away)
    returned = exchange(terms)
    return call(
        functools.partial(mix_kernel, high, wide),
        jax.ShapeDtypeStruct((tok_dev, half), BF16),
        returned,
        combine,
    )


def solution(mesh):
    side = math.isqrt(mesh.shape["ep"])
    split = Mesh(
        mesh.devices.reshape(mesh.shape["grp"], side, side, mesh.shape["tp"]),
        ("grp", "ep_0", "ep_1", "tp"),
    )
    placed = (
        P(GRP_EP, None),
        P(),
        P(GRP_EP, None),
        P(GRP_EP, None),
        P(EP, None, "tp"),
        P(EP, None, "tp"),
        P(EP, "tp", None),
        P(None, EP_TP),
        P(None, EP_TP),
        P(EP_TP, None),
        P(EP_TP),
    )

    return jax.shard_map(
        per_device, mesh=split, in_specs=placed, out_specs=P(GRP_EP, "tp"), check_vma=False
    )
```
